32 devices in a mesh: sp: 8 (over z, x), tp: 4 (over y, core).
Axes of the slice: x: 2, y: 2, z: 4, core: 2. Of those that a mesh axis runs over, the one named last changes fastest.
Arguments:
- readout_query_vectors: bfloat16 [2048, 2048], P('sp', 'tp'), may hold values from -6 to 6
- attention_key_vectors: bfloat16 [2048, 2048], P('sp', 'tp'), may hold values from -6 to 6
- attention_content_vectors: bfloat16 [2048, 2048], P('sp', 'tp'), may hold values from -6 to 6
- step_size_preactivation: bfloat16 [2048, 2048], P('sp', 'tp'), may hold values from -16 to 8
- forgetting_preactivation: float32 [2048, 2048], P('sp', 'tp'), may hold values from -22 to 3
- extra_forgetting_bias: float32 [2048, 32], P('sp', 'tp'), may hold values from -0.7 to 0
- subspace_normalizer_gain: float32 [2048], P('tp'), may hold values from 0.1 to 1.9
- skip_connection_stream: bfloat16 [2048, 2048], P('sp'), may hold values from -40 to 40
- blender_projection_matrix: bfloat16 [2048, 2048], P('tp'), may hold values from -0.125 to 0.125
- specialist_prenormal_gain: float32 [2048], replicated, may hold values from 0.1 to 1.9
- cluster_router_chance: float32 [2048], P('sp'), may hold values from 0.4 to 1
- specialist_chance_within_cluster: float32 [2048, 2], P('sp'), may hold values from 0.1 to 1
- chosen_specialist_ids: int32 [2048, 2], P('sp'), may hold values from 0 to 7, all different within a row; in each aligned block of 256 rows (0 to 255, 256 to 511, ...) at most 128 rows name the same one
- specialist_switch_matrix: bfloat16 [8, 2048, 2048], P('sp', None, 'tp'), may hold values from -0.125 to 0.125
- specialist_expansion_matrix: bfloat16 [8, 2048, 2048], P('sp', None, 'tp'), may hold values from -0.125 to 0.125
- specialist_contraction_matrix: bfloat16 [8, 2048, 2048], P('sp', 'tp'), may hold values from -0.375 to 0.375
Outputs:
- layer_out: bfloat16 [2048, 2048], P('sp')
The draws below stay inside these ranges and needn't reach their ends.
Inputs may be any that keep to these rules, and one draw needn't show every extreme that they name: `chosen_specialist_ids`: in each aligned block of 256 rows every expert is named at most 128 times.
All inputs are finite; a program needn't handle non-finite values.
Results may differ from the reference program's by a relative error of at most 0.022.
Values may be sent and summed in bfloat16 or wider, within the bound.
A program may use at most 64 MiB of HBM per device.

```python
import math
import jax
import jax.numpy as jnp
import numpy as np
from jax import lax

D = 2048
HEAD_DIM = 64
HEAD_TOTAL = 32
FF = 2048
TOP = 2
TOK_DEV = 256
TOKEN_TOTAL = 2048
EXPERTS = 8
CAP = 128
N_SP = 8
N_TP = 4


def slow_heads(key):
    chance = jax.random.uniform(jax.random.fold_in(key, 11), (HEAD_TOTAL,))
    return chance < 0.5


def draw_forgetting_preactivation(key, part):
    slow = slow_heads(key)
    head_base = jnp.where(slow, jnp.log(0.7 / TOKEN_TOTAL) + 0.5, -3.2)
    first_key = jax.random.fold_in(key, 3)
    second_key = jax.random.fold_in(key, 4)
    third_key = jax.random.fold_in(key, 5)
    jitter = 0.3 * jax.random.normal(first_key, (HEAD_TOTAL,))
    offset = jax.random.uniform(second_key, (TOKEN_TOTAL // 64, HEAD_TOTAL), minval=-0.7, maxval=0.7)
    offset = jnp.repeat(offset, 64, axis=0)
    noise_part = 0.6 * jax.random.normal(third_key, (TOKEN_TOTAL, HEAD_TOTAL, HEAD_DIM))
    result = head_base[None, :, None] + jitter[None, :, None] + offset[:, :, None] + noise_part
    return result.reshape(TOKEN_TOTAL, HEAD_TOTAL * HEAD_DIM).astype(jnp.float32)


def draw_step_size_preactivation(key, part):
    slow = slow_heads(key)
    head_base = jnp.where(slow, jnp.log(0.25 * HEAD_DIM / TOKEN_TOTAL), 0.0)
    noise_key = jax.random.fold_in(key, 6)
    noise_part = 0.8 * jax.random.normal(noise_key, (TOKEN_TOTAL, HEAD_TOTAL, HEAD_DIM))
    result = head_base[None, :, None] + noise_part
    return result.reshape(TOKEN_TOTAL, HEAD_TOTAL * HEAD_DIM).astype(jnp.bfloat16)


def draw_extra_forgetting_bias(key, part):
    spike_positions = jax.random.randint(jax.random.fold_in(key, 1), (8,), 0, TOKEN_TOTAL)
    spiked_values = jnp.any(jnp.arange(TOKEN_TOTAL)[:, None] == spike_positions[None, :], axis=1)
    spike_depth = jnp.log(jax.random.uniform(jax.random.fold_in(key, 2), (TOKEN_TOTAL, HEAD_TOTAL), minval=0.5, maxval=0.8))
    return jnp.where(spiked_values[:, None], spike_depth, 0.0).astype(jnp.float32)


def draw_skip_connection_stream(key, part):
    column = jnp.exp(jax.random.uniform(jax.random.fold_in(key, 1), (D,), minval=-0.6, maxval=0.6))
    result = jax.random.normal(jax.random.fold_in(key, 2), (TOKEN_TOTAL, D)) * column
    return result.astype(jnp.bfloat16)


def steps_of(key, extent, shards, low, top_value):
    level, own = 1.0, jax.random.fold_in(key, 6)
    for position, parts in shards:
        steps = jnp.exp(jax.random.uniform(jax.random.fold_in(own, position), (parts,), jnp.float32, low / len(shards), top_value / len(shards)))
        level = level * jnp.repeat(steps, extent[position] // parts).reshape([-1 if axis == position else 1 for axis in range(len(extent))])
    return level


def assign_block(stream_key, own, number, rows, number_of, top, limit, skew):
    order = jax.random.permutation(stream_key, number_of)
    heavy_load, common = portions_of(number_of, rows * top, limit, skew, True), portions_of(number_of, rows * top, limit, skew, False)
    places = jnp.arange(number_of)

    def named(sizes, rotation):
        used = int((sizes > 0).sum())
        fixed = max(1, used // 4)
        moved = fixed + (places - fixed + rotation * (used - fixed)) % max(1, number_of - fixed)
        return jnp.zeros((number_of,), jnp.int32).at[order[jnp.where(places < fixed, places, moved)]].set(jnp.asarray(sizes, jnp.int32))

    sizes = jnp.where(number % 4 == 0, named(heavy_load, number // 4), named(common, number - number // 4 - 1))
    mixed = jax.random.permutation(jax.random.fold_in(own, 3), number_of)
    source_of, receiver = mixed[0:number_of // 2 * 2:2], mixed[1:number_of // 2 * 2:2]
    margin = jnp.minimum(sizes[source_of] - 1, limit - sizes[receiver]) // 2
    margin = jnp.where((source_of == order[0]) | (receiver == order[0]) | (sizes[receiver] == 0), 0, jnp.maximum(margin, 0))
    moved = jax.random.randint(jax.random.fold_in(own, 4), (number_of // 2,), 0, 1 << 20) % (margin + 1)
    sizes = sizes.at[source_of].add(-moved).at[receiver].add(moved)
    members = jnp.searchsorted(jnp.cumsum(sizes), jnp.arange(rows * top), side="right").astype(jnp.int32)
    grid = members.reshape(top, rows).T
    grid = grid[jax.random.permutation(jax.random.fold_in(own, 1), rows)]
    rotation = jax.random.randint(jax.random.fold_in(own, 2), (rows, 1), 0, top)
    return jnp.take_along_axis(grid, (jnp.arange(top)[None, :] + rotation) % top, axis=1)


def portions_of(number_of, total, most, skew, full):
    loads = [(1 << 20) // math.isqrt(standing ** skew) + 1 for standing in range(1, number_of + 1)]
    largest = most if full else min(most, max(-(-total // number_of), total * loads[0] // sum(loads)))
    least = 1 if total - largest >= number_of - 1 else 0
    holding, rest = [largest] + [least] * (number_of - 1), total - largest - least * (number_of - 1)
    while rest > 0:
        free = [i for i in range(1, number_of) if holding[i] < largest] or [i for i in range(1, number_of) if holding[i] < most]
        pool, remaining = sum([loads[i] for i in free]), rest
        for i in free:
            addition = min(most - holding[i], max(1, remaining * loads[i] // pool), rest)
            holding[i] = holding[i] + addition
            rest = rest - addition
    return np.array(holding)


def centred(rng, extent, deviation, most, pieces=(), held_as=jnp.bfloat16):
    gain = steps_of(rng, extent, pieces, -0.22, 0.18) if pieces else 1.0
    values = jax.random.normal(rng, extent, jnp.float32) * deviation * gain
    return jnp.minimum(jnp.maximum(values, -most), most).astype(held_as)


def setup_inputs(seed: int = 0) -> dict:
    key_of = jax.random.split(jax.random.key(seed), 17)
    readout_query_vectors = centred(key_of[0], (TOKEN_TOTAL, D), 1.0, 6.0, ((0, 8), (1, 4)))
    attention_key_vectors = centred(key_of[1], (TOKEN_TOTAL, D), 1.0, 6.0, ((0, 8), (1, 4)))
    attention_content_vectors = centred(key_of[2], (TOKEN_TOTAL, D), 1.0, 6.0, ((0, 8), (1, 4)))
    step_size_preactivation = draw_step_size_preactivation(jax.random.fold_in(key_of[16], 71), 0)
    forgetting_preactivation = draw_forgetting_preactivation(jax.random.fold_in(key_of[16], 71), 0)
    extra_forgetting_bias = draw_extra_forgetting_bias(jax.random.fold_in(key_of[16], 71), 0)
    subspace_normalizer_gain = jnp.clip(1.0 + 0.18 * jax.random.normal(key_of[6], (D,), jnp.float32), 0.1, 1.9)
    skip_connection_stream = draw_skip_connection_stream(jax.random.fold_in(key_of[16], 71), 0)
    blender_projection_matrix = centred(key_of[8], (D, D), D ** -0.5, 0.125, ((0, 4),))
    specialist_prenormal_gain = jnp.clip(1.0 + 0.18 * jax.random.normal(key_of[9], (D,), jnp.float32), 0.1, 1.9)
    cluster_router_chance = jnp.clip(0.4 + 0.6 * jax.random.uniform(key_of[10], (TOKEN_TOTAL,), jnp.float32) ** steps_of(key_of[10], (TOKEN_TOTAL,), ((0, 8),), -0.2, 0.2), 0.4, 1.0)
    specialist_chance_within_cluster = jnp.clip(0.1 + 0.9 * jax.random.uniform(key_of[11], (TOKEN_TOTAL, TOP), jnp.float32) ** steps_of(key_of[11], (TOKEN_TOTAL, TOP), ((0, 8),), -0.2, 0.2), 0.1, 1.0)
    chosen_specialist_ids_keys = jax.random.split(jax.random.fold_in(key_of[12], 1), TOKEN_TOTAL // TOK_DEV)
    chosen_specialist_ids_turns = jax.random.permutation(jax.random.fold_in(key_of[12], 3), TOKEN_TOTAL // TOK_DEV)
    chosen_specialist_ids = jax.vmap(lambda own, number: assign_block(jax.random.fold_in(key_of[12], 2), own, number, TOK_DEV, EXPERTS, TOP, CAP, 1))(chosen_specialist_ids_keys, chosen_specialist_ids_turns).reshape((TOKEN_TOTAL, TOP))
    specialist_switch_matrix = centred(key_of[13], (EXPERTS, D, FF), D ** -0.5, 0.125, ((0, 8), (2, 4)))
    specialist_expansion_matrix = centred(key_of[14], (EXPERTS, D, FF), D ** -0.5, 0.125, ((0, 8), (2, 4)))
    specialist_contraction_matrix = centred(key_of[15], (EXPERTS, FF, D), (FF // 8) ** -0.5, 0.375, ((0, 8), (1, 4)))
    return dict(readout_query_vectors=readout_query_vectors, attention_key_vectors=attention_key_vectors, attention_content_vectors=attention_content_vectors, step_size_preactivation=step_size_preactivation, forgetting_preactivation=forgetting_preactivation, extra_forgetting_bias=extra_forgetting_bias, subspace_normalizer_gain=subspace_normalizer_gain, skip_connection_stream=skip_connection_stream, blender_projection_matrix=blender_projection_matrix, specialist_prenormal_gain=specialist_prenormal_gain, cluster_router_chance=cluster_router_chance, specialist_chance_within_cluster=specialist_chance_within_cluster, chosen_specialist_ids=chosen_specialist_ids, specialist_switch_matrix=specialist_switch_matrix, specialist_expansion_matrix=specialist_expansion_matrix, specialist_contraction_matrix=specialist_contraction_matrix)


HIGH = lax.Precision.HIGHEST

def sequence_state_blender(readout_query_vectors, attention_key_vectors, attention_content_vectors, step_size_preactivation, forgetting_preactivation, extra_forgetting_bias, subspace_normalizer_gain):
    token_count = readout_query_vectors.shape[0]
    attention_subspace_count = extra_forgetting_bias.shape[1]

    def divide_among_subspaces(data):
        return data.astype(jnp.float32).reshape(token_count, attention_subspace_count, -1)
    query_rows = divide_among_subspaces(readout_query_vectors)
    key_rows = divide_among_subspaces(attention_key_vectors)
    value_rows = divide_among_subspaces(attention_content_vectors)
    learn_rate = jax.nn.sigmoid(divide_among_subspaces(step_size_preactivation))
    logarithmic_forgetting_amounts = divide_among_subspaces(-jnp.exp(-jax.nn.softplus(-forgetting_preactivation) - 0.5)) + extra_forgetting_bias[:, :, None]
    removal = key_rows / jnp.sqrt(lax.optimization_barrier(jnp.sum(key_rows * key_rows, axis=-1, keepdims=True)) + 1e-06)
    head_dim = key_rows.shape[-1]

    def advance(state_now, inputs):
        query_t, decay_t, key_t, value_t, removal_t, rate_t = inputs
        along_removal = jnp.einsum('hvk,hk->hv', state_now, removal_t, precision=HIGH)
        state_now = state_now * jnp.exp(decay_t)[:, None, :] - along_removal[:, :, None] * (removal_t * rate_t)[:, None, :] + value_t[:, :, None] * key_t[:, None, :]
        return (state_now, jnp.einsum('hvk,hk->hv', state_now, query_t, precision=HIGH))
    initial = jnp.zeros((attention_subspace_count, head_dim, head_dim), jnp.float32)
    _, readout = lax.scan(advance, initial, (query_rows, logarithmic_forgetting_amounts, key_rows, value_rows, removal, learn_rate))
    centered = readout - lax.optimization_barrier(jnp.mean(readout, axis=-1, keepdims=True))
    spread = lax.optimization_barrier(jnp.mean(centered * centered, axis=-1, keepdims=True))
    gains = subspace_normalizer_gain.reshape(attention_subspace_count, head_dim)[None]
    normed = centered * lax.rsqrt(spread + 0.00064) * gains
    return normed.reshape(token_count, attention_subspace_count * head_dim).astype(jnp.bfloat16)

def reference(readout_query_vectors, attention_key_vectors, attention_content_vectors, step_size_preactivation, forgetting_preactivation, extra_forgetting_bias, subspace_normalizer_gain, skip_connection_stream, blender_projection_matrix, specialist_prenormal_gain, cluster_router_chance, specialist_chance_within_cluster, chosen_specialist_ids, specialist_switch_matrix, specialist_expansion_matrix, specialist_contraction_matrix):
    blender_result = sequence_state_blender(readout_query_vectors, attention_key_vectors, attention_content_vectors, step_size_preactivation, forgetting_preactivation, extra_forgetting_bias, subspace_normalizer_gain)
    token_count = blender_result.shape[0]
    group_rows = D // N_TP

    def add_group(running, group):
        first_row = (group * group_rows).astype(jnp.int32)
        columns = lax.dynamic_slice_in_dim(blender_result, first_row, group_rows, 1)
        weight_rows = lax.dynamic_slice_in_dim(blender_projection_matrix, first_row, group_rows, 0)
        term = jnp.dot(columns, weight_rows, preferred_element_type=jnp.float32)
        rounded = lax.optimization_barrier(term.astype(jnp.bfloat16)).astype(jnp.float32)
        return (running + rounded, None)
    branch, _ = lax.scan(add_group, jnp.zeros((token_count, D), jnp.float32), jnp.arange(N_TP, dtype=jnp.int32))
    hidden_state = skip_connection_stream.astype(jnp.float32) + branch
    inverse_rms = lax.rsqrt(lax.optimization_barrier(jnp.mean(hidden_state * hidden_state, axis=1, keepdims=True)) + 1e-06)
    normed = (hidden_state * inverse_rms * specialist_prenormal_gain).astype(jnp.bfloat16)
    flat_expert = chosen_specialist_ids.reshape(N_SP, TOK_DEV * TOP)
    one_hot = (flat_expert[:, :, None] == jnp.arange(EXPERTS, dtype=jnp.int32)[None, None, :]).astype(jnp.int32)
    earlier = lax.optimization_barrier(jnp.sum((jnp.cumsum(one_hot, axis=1) - one_hot) * one_hot, axis=2))
    source = jnp.arange(N_SP, dtype=jnp.int32)[:, None]
    slot_index = (flat_expert * (N_SP * CAP) + source * CAP + earlier).reshape(-1)
    token_of = jnp.arange(N_SP * TOK_DEV * TOP, dtype=jnp.int32) // TOP
    slot_owner = jnp.full((EXPERTS * N_SP * CAP,), N_SP * TOK_DEV, jnp.int32).at[slot_index].set(token_of)
    padded = jnp.concatenate([normed, jnp.zeros((1, D), jnp.bfloat16)], axis=0)

    def expert_rows(operands):
        owners, w_gate, w_up, w_down = operands
        rows_in = padded[owners]
        gate_act = jnp.dot(rows_in, w_gate, preferred_element_type=jnp.float32)
        upward = jnp.dot(rows_in, w_up, preferred_element_type=jnp.float32)
        hidden = (jax.nn.silu(gate_act) * upward).astype(jnp.bfloat16)
        unit_group = w_down.shape[0] // N_TP
        hidden_split = hidden.astype(jnp.float32).reshape(-1, N_TP, unit_group)
        down_split = w_down.astype(jnp.float32).reshape(N_TP, unit_group, D)
        partial_value = jnp.einsum('rtf,tfd->trd', hidden_split, down_split)
        rounded = lax.optimization_barrier(partial_value.astype(jnp.bfloat16)).astype(jnp.float32)
        return lax.optimization_barrier(jnp.sum(rounded, axis=0))
    results = lax.map(expert_rows, (slot_owner.reshape(EXPERTS, N_SP * CAP), specialist_switch_matrix, specialist_expansion_matrix, specialist_contraction_matrix))
    picked = results.reshape(-1, D)[slot_index].reshape(N_SP * TOK_DEV, TOP, D)
    route_weight = cluster_router_chance[:, None] * specialist_chance_within_cluster / lax.optimization_barrier(jnp.sum(specialist_chance_within_cluster, axis=1, keepdims=True))
    mixture = lax.optimization_barrier(jnp.sum(route_weight[:, :, None] * picked, axis=1))
    return (hidden_state + mixture).astype(jnp.bfloat16)
```

```python
import functools

import jax
import jax.numpy as jnp
from jax import lax
from jax.experimental import pallas as pl
from jax.experimental.pallas import tpu as pltpu
from jax.sharding import PartitionSpec as P

MESH = pl.DeviceIdType.MESH
F32 = jnp.float32
BF16 = jnp.bfloat16


def dot(left, right, axes=(1, 0)):
    return lax.dot_general(
        left, right, (((axes[0],), (axes[1],)), ((), ())), preferred_element_type=F32
    )


def halves(data):
    high = data.astype(BF16)
    return high, (data - high.astype(F32)).astype(BF16)


def dot3(left, right, axes=(1, 0)):
    lh, ll = halves(left)
    rh, rl = halves(right)
    return dot(lh, rh, axes) + (dot(lh, rl, axes) + dot(ll, rh, axes))


def dot1(left, right, axes=(1, 0)):
    return dot(left.astype(BF16), right.astype(BF16), axes)


def mixer_kernel(head_dim, segment, q_ref, k_ref, v_ref, a_ref, f_ref, b_ref, out_ref, map_ref, ka_ref):
    pair = pl.program_id(0)
    rows, width = q_ref.shape
    blocks = rows // segment
    per = width // head_dim
    shift = segment.bit_length() - 1
    row = lax.broadcasted_iota(jnp.int32, (rows, rows), 0)
    col = lax.broadcasted_iota(jnp.int32, (rows, rows), 1)
    same = (row >> shift) == (col >> shift)
    strict = same & (row > col)
    inclusive = same & (row >= col)
    triangle = jnp.where(inclusive, 1.0, 0.0).astype(BF16)
    lane = lax.broadcasted_iota(jnp.int32, (rows, width), 1)
    bias = b_ref[...]
    bias_lane = lax.broadcasted_iota(jnp.int32, bias.shape, 1)

    def spread(values):
        total = values[per - 1]
        for h in range(per - 2, -1, -1):
            total = jnp.where(lane < (h + 1) * head_dim, values[h], total)
        return total

    own_bias = [
        jnp.sum(jnp.where(bias_lane == pair * per + h, bias, 0.0), axis=1, keepdims=True)
        for h in range(per)
    ]
    decay = -(0.6065306597126334 / (1.0 + jnp.exp(-f_ref[...]))) + spread(own_bias)
    high, low = halves(decay)
    lowest = (decay - high.astype(F32) - low.astype(F32)).astype(BF16)
    cumulative = dot(triangle, high) + (dot(triangle, low) + dot(triangle, lowest))
    closing_rows = cumulative.reshape(blocks, segment, width)[:, segment - 1 :, :]
    closing = jnp.broadcast_to(closing_rows, (blocks, segment, width)).reshape(rows, width)
    keys = k_ref[...].astype(F32)
    squares = keys * keys
    norms = spread(
        [
            jnp.sum(squares[:, h * head_dim : (h + 1) * head_dim], axis=1, keepdims=True)
            for h in range(per)
        ]
    )
    removal = keys * lax.rsqrt(norms + 1e-06)
    rate = 1.0 / (1.0 + jnp.exp(-a_ref[...].astype(F32)))
    beta = removal * rate
    grow = jnp.exp(-cumulative)
    fade = jnp.exp(closing - cumulative)
    alpha_all = -removal * jnp.exp(cumulative - decay)
    beta_hat_all = beta * grow
    key_hat_all = keys * grow
    query_all = q_ref[...].astype(F32) * jnp.exp(cumulative)
    beta_bar_all = beta * fade
    key_bar_all = keys * fade
    values_all = v_ref[...]
    keep_all = jnp.exp(closing_rows)
    eye = lax.broadcasted_iota(jnp.int32, (head_dim, head_dim), 0) == lax.broadcasted_iota(
        jnp.int32, (head_dim, head_dim), 1
    )
    outs, maps = [], []
    for h in range(per):
        part = slice(h * head_dim, (h + 1) * head_dim)
        alpha, beta_hat, key_hat = alpha_all[:, part], beta_hat_all[:, part], key_hat_all[:, part]
        query, values = query_all[:, part], values_all[:, part]
        beta_bar, key_bar = beta_bar_all[:, part], key_bar_all[:, part]
        lower = jnp.where(strict, dot3(alpha, beta_hat, (1, 1)), 0.0)
        remove_write = jnp.where(strict, dot3(alpha, key_hat, (1, 1)), 0.0)
        read_remove = jnp.where(inclusive, dot1(query, beta_hat, (1, 1)), 0.0)
        read_write = jnp.where(inclusive, dot1(query, key_hat, (1, 1)), 0.0)
        inverse = jnp.where(row == col, 1.0, jnp.where((row >> 1) == (col >> 1), lower, 0.0))
        for s in range(1, shift):
            off = ((row >> (s + 1)) == (col >> (s + 1))) & ((row >> s) != (col >> s))
            inverse = inverse + dot3(inverse, dot3(jnp.where(off, lower, 0.0), inverse))
        wh, wl = halves(remove_write)
        side = jnp.concatenate([alpha, dot(wh, values) + dot(wl, values)], axis=1)
        solved = dot3(inverse, side)
        read = dot1(read_remove, solved)
        read_map = query + read[:, :head_dim]
        local = read[:, head_dim:] + dot(read_write.astype(BF16), values)
        state = jnp.concatenate(
            [jnp.where(eye, 1.0, 0.0), jnp.zeros((head_dim, head_dim), F32)], axis=0
        )
        out_rows, map_rows = [], []
        for b in range(blocks):
            at = slice(b * segment, (b + 1) * segment)
            seen = dot1(read_map[at], state, (1, 1))
            map_rows.append(seen[:, :head_dim])
            out_rows.append(local[at] + seen[:, head_dim:])
            step = dot3(solved[at], beta_bar[at], (0, 0))
            bh, bl = halves(key_bar[at])
            add = step[head_dim:] + dot(values[at], bh, (0, 0)) + dot(values[at], bl, (0, 0))
            keep = step[:head_dim] + jnp.where(eye, keep_all[b][:, part], 0.0)
            state = dot3(state, keep)
            state = jnp.concatenate([state[:head_dim], state[head_dim:] + add], axis=0)
        outs.append(jnp.concatenate(out_rows, axis=0))
        maps.append(jnp.concatenate(map_rows, axis=0))
        ka_ref[h] = jnp.concatenate([state[:head_dim], state[head_dim:]], axis=1).astype(BF16)
    out_ref[...] = jnp.concatenate(outs, axis=1)
    map_ref[...] = jnp.concatenate(maps, axis=1).astype(BF16)


def exchange_kernel(count, per, workers, ka_ref, st_ref, got, fold, send1, recv1, send2, recv2):
    me = lax.axis_index("sp")
    dim = ka_ref.shape[1]
    barrier = pltpu.get_barrier_semaphore()
    for d in range(1, count):
        pl.semaphore_signal(
            barrier, inc=1, device_id={"sp": lax.rem(me + d, count)}, device_id_type=MESH
        )
    pl.semaphore_wait(barrier, count - 1)

    def first(t, owner):
        return pltpu.make_async_remote_copy(
            src_ref=ka_ref.at[pl.ds(t * per, per)],
            dst_ref=got.at[owner],
            send_sem=send1.at[t],
            recv_sem=recv1.at[owner],
            device_id={"sp": t},
            device_id_type=MESH,
        )

    def second(t, owner):
        return pltpu.make_async_remote_copy(
            src_ref=fold.at[t],
            dst_ref=st_ref.at[pl.ds(owner * per, per)],
            send_sem=send2.at[t],
            recv_sem=recv2.at[owner],
            device_id={"sp": t},
            device_id_type=MESH,
        )

    for t in range(workers):
        @pl.when(t != me)
        def _(t=t):
            first(t, me).start()

    def work():
        got[me] = ka_ref[pl.ds(me * per, per)]
        state = [jnp.zeros((dim, dim), F32) for _ in range(per)]
        for j in range(count):
            @pl.when(j != me)
            def _(j=j):
                pltpu.make_async_remote_copy(
                    src_ref=got.at[j],
                    dst_ref=got.at[j],
                    send_sem=send1.at[0],
                    recv_sem=recv1.at[j],
                    device_id={"sp": j},
                    device_id_type=MESH,
                ).wait_recv()
            for i in range(per):
                fold[j, i] = jnp.concatenate([state[i], jnp.zeros_like(state[i])], axis=1).astype(BF16)
                both = got[j, i]
                keep, add = both[:, :dim], both[:, dim:].astype(F32)
                sh, sl = halves(state[i])
                state[i] = dot(sh, keep) + dot(sl, keep) + add
        for t in range(count):
            @pl.when(t != me)
            def _(t=t):
                second(t, me).start()
        st_ref[pl.ds(me * per, per)] = fold[me]
        for t in range(count):
            @pl.when(t != me)
            def _(t=t):
                second(t, me).wait_send()

    if workers == count:
        work()
    else:
        pl.when(me < workers)(work)
    for t in range(workers):
        @pl.when(t != me)
        def _(t=t):
            first(t, me).wait_send()
            pltpu.make_async_remote_copy(
                src_ref=fold.at[t],
                dst_ref=st_ref.at[pl.ds(t * per, per)],
                send_sem=send2.at[0],
                recv_sem=recv2.at[t],
                device_id={"sp": t},
                device_id_type=MESH,
            ).wait_recv()


def finish_kernel(head_dim, out_ref, map_ref, st_ref, gain_ref, w_ref, part_ref, mixed):
    @pl.when(pl.program_id(0) == 0)
    def _():
        for h in range(out_ref.shape[1] // head_dim):
            part = slice(h * head_dim, (h + 1) * head_dim)
            states = st_ref[h][:, :head_dim]
            output = out_ref[:, part] + dot(map_ref[:, part], states, (1, 1))
            centered = output - jnp.mean(output, axis=1, keepdims=True)
            spread = jnp.mean(centered * centered, axis=1, keepdims=True)
            mixed[:, part] = (centered * lax.rsqrt(spread + 0.00064) * gain_ref[:, part]).astype(BF16)

    part_ref[...] = dot(mixed[...], w_ref[...]).astype(BF16)


def mixer_branch(query, key, value, step, forget, bias, gain, blender):
    count = lax.axis_size("sp")
    rows, channels = query.shape
    heads = bias.shape[1]
    head_dim = channels // heads
    segment = min(64, rows)
    width = 2 * head_dim
    pairs = heads // 2
    block = pl.BlockSpec((rows, width), lambda p: (0, p))
    out, maps, ka = pl.pallas_call(
        functools.partial(mixer_kernel, head_dim, segment),
        grid=(pairs,),
        in_specs=[block] * 5 + [pl.BlockSpec((rows, heads), lambda p: (0, 0))],
        out_specs=[block, block, pl.BlockSpec((2, head_dim, width), lambda p: (p, 0, 0))],
        out_shape=[
            jax.ShapeDtypeStruct((rows, channels), F32),
            jax.ShapeDtypeStruct((rows, channels), BF16),
            jax.ShapeDtypeStruct((heads, head_dim, width), BF16),
        ],
        compiler_params=pltpu.CompilerParams(vmem_limit_bytes=50 * 1024 * 1024),
    )(query, key, value, step, forget, bias)
    per = max(1, heads // count)
    workers = heads // per
    vmem = pl.BlockSpec(memory_space=pltpu.VMEM)
    states = pl.pallas_call(
        functools.partial(exchange_kernel, count, per, workers),
        out_shape=jax.ShapeDtypeStruct((heads, head_dim, width), BF16),
        in_specs=[vmem],
        out_specs=vmem,
        scratch_shapes=[
            pltpu.VMEM((count, per, head_dim, width), BF16),
            pltpu.VMEM((count, per, head_dim, width), BF16),
            pltpu.SemaphoreType.DMA((count,)),
            pltpu.SemaphoreType.DMA((count,)),
            pltpu.SemaphoreType.DMA((count,)),
            pltpu.SemaphoreType.DMA((count,)),
        ],
        compiler_params=pltpu.CompilerParams(collective_id=1, has_side_effects=True),
    )(ka)
    model_width = blender.shape[1]
    tile = min(512, model_width)
    whole = lambda *shape: pl.BlockSpec(shape, lambda p: (0,) * len(shape))
    return pl.pallas_call(
        functools.partial(finish_kernel, head_dim),
        grid=(model_width // tile,),
        in_specs=[
            whole(rows, channels),
            whole(rows, channels),
            whole(heads, head_dim, width),
            whole(1, channels),
            pl.BlockSpec((channels, tile), lambda p: (0, p)),
        ],
        out_specs=pl.BlockSpec((rows, tile), lambda p: (0, p)),
        out_shape=jax.ShapeDtypeStruct((rows, model_width), BF16),
        scratch_shapes=[pltpu.VMEM((rows, channels), BF16)],
    )(out, maps, states, gain.reshape(1, channels), blender)


def body(
    readout_query_vectors,
    attention_key_vectors,
    attention_content_vectors,
    step_size_preactivation,
    forgetting_preactivation,
    extra_forgetting_bias,
    subspace_normalizer_gain,
    skip_connection_stream,
    blender_projection_matrix,
    specialist_prenormal_gain,
    cluster_router_chance,
    specialist_chance_within_cluster,
    chosen_specialist_ids,
    specialist_switch_matrix,
    specialist_expansion_matrix,
    specialist_contraction_matrix,
):
    partial_branch = mixer_branch(
        readout_query_vectors,
        attention_key_vectors,
        attention_content_vectors,
        step_size_preactivation,
        forgetting_preactivation,
        extra_forgetting_bias,
        subspace_normalizer_gain,
        blender_projection_matrix,
    )
    branch = lax.psum(partial_branch, "tp").astype(jnp.float32)
    hidden_state = skip_connection_stream.astype(jnp.float32) + branch
    inverse_rms = lax.rsqrt(jnp.mean(hidden_state * hidden_state, axis=1, keepdims=True) + 1e-06)
    normed = (hidden_state * inverse_rms * specialist_prenormal_gain).astype(jnp.bfloat16)
    tok_rows = skip_connection_stream.shape[0]
    model_width = skip_connection_stream.shape[1]
    local_experts = specialist_switch_matrix.shape[0]
    experts = local_experts * lax.axis_size("sp")
    top_count = chosen_specialist_ids.shape[1]
    capacity = 2 * tok_rows * top_count // experts
    flat_expert = chosen_specialist_ids.reshape(-1)
    one_hot = (flat_expert[:, None] == jnp.arange(experts, dtype=jnp.int32)[None, :]).astype(
        jnp.int32
    )
    earlier = jnp.sum((jnp.cumsum(one_hot, axis=0) - one_hot) * one_hot, axis=1)
    slot_index = flat_expert * capacity + earlier
    token_of = jnp.arange(flat_expert.shape[0], dtype=jnp.int32) // top_count
    slot_owner = jnp.full((experts * capacity,), tok_rows, jnp.int32).at[slot_index].set(token_of)
    padded = jnp.concatenate([normed, jnp.zeros((1, model_width), jnp.bfloat16)], axis=0)
    outgoing = padded[slot_owner].reshape(experts, capacity, model_width)
    route_weight = (
        cluster_router_chance[:, None]
        * specialist_chance_within_cluster
        / jnp.sum(specialist_chance_within_cluster, axis=1, keepdims=True)
    )
    rows_in = lax.all_to_all(outgoing, "sp", split_axis=0, concat_axis=0, tiled=True)
    grouped = rows_in.reshape(-1, local_experts, rows_in.shape[1], model_width)
    gate_act = jnp.einsum(
        "secd,edf->secf", grouped, specialist_switch_matrix, preferred_element_type=jnp.float32
    )
    upward = jnp.einsum(
        "secd,edf->secf", grouped, specialist_expansion_matrix, preferred_element_type=jnp.float32
    )
    hidden = (jax.nn.silu(gate_act) * upward).astype(jnp.bfloat16)
    partial_value = jnp.einsum(
        "secf,efd->secd", hidden, specialist_contraction_matrix, preferred_element_type=jnp.float32
    )
    partial_value = partial_value.astype(jnp.bfloat16).reshape(rows_in.shape)
    summed = lax.psum_scatter(
        partial_value.astype(jnp.float32).astype(jnp.bfloat16),
        "tp",
        scatter_dimension=2,
        tiled=True,
    ).astype(jnp.float32)
    returned = lax.all_to_all(
        summed.astype(jnp.bfloat16), "sp", split_axis=0, concat_axis=0, tiled=True
    ).astype(summed.dtype)
    column_count = returned.shape[2]
    picked = returned.reshape(experts * capacity, column_count)[slot_index].reshape(
        tok_rows, top_count, column_count
    )
    mixture = jnp.sum(route_weight[:, :, None] * picked, axis=1)
    own_columns = lax.dynamic_slice_in_dim(
        hidden_state, lax.axis_index("tp") * column_count, column_count, 1
    )
    return lax.all_gather((own_columns + mixture).astype(jnp.bfloat16), "tp", axis=1, tiled=True)


def solution(mesh):
    in_specs = (
        P("sp", "tp"),
        P("sp", "tp"),
        P("sp", "tp"),
        P("sp", "tp"),
        P("sp", "tp"),
        P("sp", "tp"),
        P("tp"),
        P("sp", None),
        P("tp", None),
        P(),
        P("sp"),
        P("sp", None),
        P("sp", None),
        P("sp", None, "tp"),
        P("sp", None, "tp"),
        P("sp", "tp", None),
    )
    out_specs = P("sp", None)
    return jax.shard_map(body, mesh=mesh, in_specs=in_specs, out_specs=out_specs, check_vma=False)
```

```python
import functools

import jax
import jax.numpy as jnp
from jax import lax
from jax.experimental import pallas as pl
from jax.experimental.pallas import tpu as pltpu
from jax.sharding import PartitionSpec as P

MESH = pl.DeviceIdType.MESH
F32 = jnp.float32
BF16 = jnp.bfloat16


def dot(left, right, axes=(1, 0)):
    return lax.dot_general(
        left, right, (((axes[0],), (axes[1],)), ((), ())), preferred_element_type=F32
    )


def halves(data):
    high = data.astype(BF16)
    return high, (data - high.astype(F32)).astype(BF16)


def dot3(left, right, axes=(1, 0)):
    lh, ll = halves(left)
    rh, rl = halves(right)
    return dot(lh, rh, axes) + (dot(lh, rl, axes) + dot(ll, rh, axes))


def dot1(left, right, axes=(1, 0)):
    return dot(left.astype(BF16), right.astype(BF16), axes)


def mixer_kernel(head_dim, segment, q_ref, k_ref, v_ref, a_ref, f_ref, b_ref, out_ref, map_ref, ka_ref):
    pair = pl.program_id(0)
    rows, width = q_ref.shape
    blocks = rows // segment
    per = width // head_dim
    shift = segment.bit_length() - 1
    row = lax.broadcasted_iota(jnp.int32, (rows, rows), 0)
    col = lax.broadcasted_iota(jnp.int32, (rows, rows), 1)
    same = (row >> shift) == (col >> shift)
    strict = same & (row > col)
    inclusive = same & (row >= col)
    triangle = jnp.where(inclusive, 1.0, 0.0).astype(BF16)
    lane = lax.broadcasted_iota(jnp.int32, (rows, width), 1)
    bias = b_ref[...]
    bias_lane = lax.broadcasted_iota(jnp.int32, bias.shape, 1)

    def spread(values):
        total = values[per - 1]
        for h in range(per - 2, -1, -1):
            total = jnp.where(lane < (h + 1) * head_dim, values[h], total)
        return total

    own_bias = [
        jnp.sum(jnp.where(bias_lane == pair * per + h, bias, 0.0), axis=1, keepdims=True)
        for h in range(per)
    ]
    decay = -(0.6065306597126334 / (1.0 + jnp.exp(-f_ref[...]))) + spread(own_bias)
    high, low = halves(decay)
    lowest = (decay - high.astype(F32) - low.astype(F32)).astype(BF16)
    cumulative = dot(triangle, high) + (dot(triangle, low) + dot(triangle, lowest))
    closing_rows = cumulative.reshape(blocks, segment, width)[:, segment - 1 :, :]
    closing = jnp.broadcast_to(closing_rows, (blocks, segment, width)).reshape(rows, width)
    keys = k_ref[...].astype(F32)
    squares = keys * keys
    norms = spread(
        [
            jnp.sum(squares[:, h * head_dim : (h + 1) * head_dim], axis=1, keepdims=True)
            for h in range(per)
        ]
    )
    removal = keys * lax.rsqrt(norms + 1e-06)
    rate = 1.0 / (1.0 + jnp.exp(-a_ref[...].astype(F32)))
    beta = removal * rate
    grow = jnp.exp(-cumulative)
    fade = jnp.exp(closing - cumulative)
    alpha_all = -removal * jnp.exp(cumulative - decay)
    beta_hat_all = beta * grow
    key_hat_all = keys * grow
    query_all = q_ref[...].astype(F32) * jnp.exp(cumulative)
    beta_bar_all = beta * fade
    key_bar_all = keys * fade
    values_all = v_ref[...]
    keep_all = jnp.exp(closing_rows)
    eye = lax.broadcasted_iota(jnp.int32, (head_dim, head_dim), 0) == lax.broadcasted_iota(
        jnp.int32, (head_dim, head_dim), 1
    )
    outs, maps = [], []
    for h in range(per):
        part = slice(h * head_dim, (h + 1) * head_dim)
        alpha, beta_hat, key_hat = alpha_all[:, part], beta_hat_all[:, part], key_hat_all[:, part]
        query, values = query_all[:, part], values_all[:, part]
        beta_bar, key_bar = beta_bar_all[:, part], key_bar_all[:, part]
        lower = jnp.where(strict, dot3(alpha, beta_hat, (1, 1)), 0.0)
        remove_write = jnp.where(strict, dot3(alpha, key_hat, (1, 1)), 0.0)
        read_remove = jnp.where(inclusive, dot1(query, beta_hat, (1, 1)), 0.0)
        read_write = jnp.where(inclusive, dot1(query, key_hat, (1, 1)), 0.0)
        inverse = jnp.where(row == col, 1.0, jnp.where((row >> 1) == (col >> 1), lower, 0.0))
        for s in range(1, shift):
            off = ((row >> (s + 1)) == (col >> (s + 1))) & ((row >> s) != (col >> s))
            inverse = inverse + dot3(inverse, dot3(jnp.where(off, lower, 0.0), inverse))
        wh, wl = halves(remove_write)
        side = jnp.concatenate([alpha, dot(wh, values) + dot(wl, values)], axis=1)
        solved = dot3(inverse, side)
        read = dot1(read_remove, solved)
        read_map = query + read[:, :head_dim]
        local = read[:, head_dim:] + dot(read_write.astype(BF16), values)
        state = jnp.concatenate(
            [jnp.where(eye, 1.0, 0.0), jnp.zeros((head_dim, head_dim), F32)], axis=0
        )
        out_rows, map_rows = [], []
        for b in range(blocks):
            at = slice(b * segment, (b + 1) * segment)
            seen = dot1(read_map[at], state, (1, 1))
            map_rows.append(seen[:, :head_dim])
            out_rows.append(local[at] + seen[:, head_dim:])
            step = dot3(solved[at], beta_bar[at], (0, 0))
            bh, bl = halves(key_bar[at])
            add = step[head_dim:] + dot(values[at], bh, (0, 0)) + dot(values[at], bl, (0, 0))
            keep = step[:head_dim] + jnp.where(eye, keep_all[b][:, part], 0.0)
            state = dot3(state, keep)
            state = jnp.concatenate([state[:head_dim], state[head_dim:] + add], axis=0)
        outs.append(jnp.concatenate(out_rows, axis=0))
        maps.append(jnp.concatenate(map_rows, axis=0))
        ka_ref[h] = jnp.concatenate([state[:head_dim], state[head_dim:]], axis=1).astype(BF16)
    out_ref[...] = jnp.concatenate(outs, axis=1)
    map_ref[...] = jnp.concatenate(maps, axis=1).astype(BF16)


def exchange_kernel(count, per, workers, ka_ref, st_ref, got, fold, send1, recv1, send2, recv2):
    me = lax.axis_index("sp")
    dim = ka_ref.shape[1]
    barrier = pltpu.get_barrier_semaphore()
    for d in range(1, count):
        pl.semaphore_signal(
            barrier, inc=1, device_id={"sp": lax.rem(me + d, count)}, device_id_type=MESH
        )
    pl.semaphore_wait(barrier, count - 1)

    def first(t, owner):
        return pltpu.make_async_remote_copy(
            src_ref=ka_ref.at[pl.ds(t * per, per)],
            dst_ref=got.at[owner],
            send_sem=send1.at[t],
            recv_sem=recv1.at[owner],
            device_id={"sp": t},
            device_id_type=MESH,
        )

    def second(t, owner):
        return pltpu.make_async_remote_copy(
            src_ref=fold.at[t],
            dst_ref=st_ref.at[pl.ds(owner * per, per)],
            send_sem=send2.at[t],
            recv_sem=recv2.at[owner],
            device_id={"sp": t},
            device_id_type=MESH,
        )

    for t in range(workers):
        @pl.when(t != me)
        def _(t=t):
            first(t, me).start()

    def work():
        got[me] = ka_ref[pl.ds(me * per, per)]
        state = [jnp.zeros((dim, dim), F32) for _ in range(per)]
        for j in range(count):
            @pl.when(j != me)
            def _(j=j):
                pltpu.make_async_remote_copy(
                    src_ref=got.at[j],
                    dst_ref=got.at[j],
                    send_sem=send1.at[0],
                    recv_sem=recv1.at[j],
                    device_id={"sp": j},
                    device_id_type=MESH,
                ).wait_recv()
            for i in range(per):
                fold[j, i] = jnp.concatenate([state[i], jnp.zeros_like(state[i])], axis=1).astype(BF16)
                both = got[j, i]
                keep, add = both[:, :dim], both[:, dim:].astype(F32)
                sh, sl = halves(state[i])
                state[i] = dot(sh, keep) + dot(sl, keep) + add
        for t in range(count):
            @pl.when(t != me)
            def _(t=t):
                second(t, me).start()
        st_ref[pl.ds(me * per, per)] = fold[me]
        for t in range(count):
            @pl.when(t != me)
            def _(t=t):
                second(t, me).wait_send()

    if workers == count:
        work()
    else:
        pl.when(me < workers)(work)
    for t in range(workers):
        @pl.when(t != me)
        def _(t=t):
            first(t, me).wait_send()
            pltpu.make_async_remote_copy(
                src_ref=fold.at[t],
                dst_ref=st_ref.at[pl.ds(t * per, per)],
                send_sem=send2.at[0],
                recv_sem=recv2.at[t],
                device_id={"sp": t},
                device_id_type=MESH,
            ).wait_recv()


def finish_kernel(head_dim, out_ref, map_ref, st_ref, gain_ref, w_ref, part_ref, mixed):
    @pl.when(pl.program_id(0) == 0)
    def _():
        for h in range(out_ref.shape[1] // head_dim):
            part = slice(h * head_dim, (h + 1) * head_dim)
            states = st_ref[h][:, :head_dim]
            output = out_ref[:, part] + dot(map_ref[:, part], states, (1, 1))
            centered = output - jnp.mean(output, axis=1, keepdims=True)
            spread = jnp.mean(centered * centered, axis=1, keepdims=True)
            mixed[:, part] = (centered * lax.rsqrt(spread + 0.00064) * gain_ref[:, part]).astype(BF16)

    part_ref[...] = dot(mixed[...], w_ref[...]).astype(BF16)


def mixer_branch(query, key, value, step, forget, bias, gain, blender):
    count = lax.axis_size("sp")
    rows, channels = query.shape
    heads = bias.shape[1]
    head_dim = channels // heads
    segment = min(64, rows)
    width = 2 * head_dim
    pairs = heads // 2
    block = pl.BlockSpec((rows, width), lambda p: (0, p))
    out, maps, ka = pl.pallas_call(
        functools.partial(mixer_kernel, head_dim, segment),
        grid=(pairs,),
        in_specs=[block] * 5 + [pl.BlockSpec((rows, heads), lambda p: (0, 0))],
        out_specs=[block, block, pl.BlockSpec((2, head_dim, width), lambda p: (p, 0, 0))],
        out_shape=[
            jax.ShapeDtypeStruct((rows, channels), F32),
            jax.ShapeDtypeStruct((rows, channels), BF16),
            jax.ShapeDtypeStruct((heads, head_dim, width), BF16),
        ],
        compiler_params=pltpu.CompilerParams(vmem_limit_bytes=50 * 1024 * 1024),
    )(query, key, value, step, forget, bias)
    per = max(1, heads // count)
    workers = heads // per
    vmem = pl.BlockSpec(memory_space=pltpu.VMEM)
    states = pl.pallas_call(
        functools.partial(exchange_kernel, count, per, workers),
        out_shape=jax.ShapeDtypeStruct((heads, head_dim, width), BF16),
        in_specs=[vmem],
        out_specs=vmem,
        scratch_shapes=[
            pltpu.VMEM((count, per, head_dim, width), BF16),
            pltpu.VMEM((count, per, head_dim, width), BF16),
            pltpu.SemaphoreType.DMA((count,)),
            pltpu.SemaphoreType.DMA((count,)),
            pltpu.SemaphoreType.DMA((count,)),
            pltpu.SemaphoreType.DMA((count,)),
        ],
        compiler_params=pltpu.CompilerParams(collective_id=1, has_side_effects=True),
    )(ka)
    model_width = blender.shape[1]
    tile = min(512, model_width)
    whole = lambda *shape: pl.BlockSpec(shape, lambda p: (0,) * len(shape))
    return pl.pallas_call(
        functools.partial(finish_kernel, head_dim),
        grid=(model_width // tile,),
        in_specs=[
            whole(rows, channels),
            whole(rows, channels),
            whole(heads, head_dim, width),
            whole(1, channels),
            pl.BlockSpec((channels, tile), lambda p: (0, p)),
        ],
        out_specs=pl.BlockSpec((rows, tile), lambda p: (0, p)),
        out_shape=jax.ShapeDtypeStruct((rows, model_width), BF16),
        scratch_shapes=[pltpu.VMEM((rows, channels), BF16)],
    )(out, maps, states, gain.reshape(1, channels), blender)


def greet(sp_count, tp_count, sp, tp):
    barrier = pltpu.get_barrier_semaphore()
    for d in range(1, sp_count):
        pl.semaphore_signal(
            barrier, inc=1, device_id={"sp": lax.rem(sp + d, sp_count)}, device_id_type=MESH
        )
    for d in range(1, tp_count):
        pl.semaphore_signal(
            barrier, inc=1, device_id={"tp": lax.rem(tp + d, tp_count)}, device_id_type=MESH
        )
    pl.semaphore_wait(barrier, sp_count + tp_count - 2)


def copy_to(src, dst, send, recv, device):
    return pltpu.make_async_remote_copy(
        src_ref=src,
        dst_ref=dst,
        send_sem=send,
        recv_sem=recv,
        device_id=device,
        device_id_type=MESH,
    )


def span(index, size):
    return pl.ds(pl.multiple_of(index * size, size), size)


def row_total(data, terms):
    ones = jnp.ones((8, data.shape[1]), BF16)
    total = None
    for _ in range(terms):
        piece = data.astype(BF16)
        data = data - piece.astype(F32)
        product = dot(ones, piece, (1, 1))
        total = product if total is None else total + product
    return total


def route_kernel(
    sp_count, tp_count, experts, capacity,
    part_ref, skip_ref, gain_ref, ids_ref,
    hidden_ref, slot_ref, rows_ref,
    gathered, squares, outgoing,
    s_part, r_part, s_sq, r_sq, s_out, r_out, s_own, s_fwd, r_col,
):
    sp, tp = lax.axis_index("sp"), lax.axis_index("tp")
    rows, model = part_ref.shape
    cols = model // tp_count
    mine = span(tp, cols)
    groups = tp_count // 2
    core, group = lax.rem(tp, 2), tp // 2
    sibling = group * 2 + 1 - core
    greet(sp_count, tp_count, sp, tp)

    def part_copy(p):
        return copy_to(
            part_ref.at[:, span(p, cols)], gathered.at[tp], s_part.at[p], r_part.at[tp], {"tp": p}
        )

    for d in range(1, tp_count):
        part_copy(lax.rem(tp + d, tp_count)).start()

    ids = ids_ref[...]
    top = ids.shape[1]
    lanes = lax.broadcasted_iota(jnp.int32, (rows, experts), 1)
    named = [ids[:, k : k + 1] == lanes for k in range(top)]
    anyone = sum(jnp.where(n, 1.0, 0.0) for n in named).astype(BF16)
    r0 = lax.broadcasted_iota(jnp.int32, (rows, rows), 0)
    r1 = lax.broadcasted_iota(jnp.int32, (rows, rows), 1)
    before = dot(jnp.where(r0 > r1, 1.0, 0.0).astype(BF16), anyone)
    slots = [
        jnp.sum(
            jnp.where(n, before + lanes.astype(F32) * capacity, 0.0), axis=1, keepdims=True
        ).astype(jnp.int32)
        for n in named
    ]
    slot_ref[...] = jnp.concatenate(slots, axis=1)

    branch = part_ref[:, mine].astype(F32)
    for d in range(1, tp_count):
        p = lax.rem(tp + d, tp_count)
        copy_to(gathered.at[p], gathered.at[p], s_part.at[p], r_part.at[p], {"tp": p}).wait_recv()
        branch = branch + gathered[p].astype(F32)
    hidden = skip_ref[:, mine].astype(F32) + branch
    hidden_ref[...] = hidden
    squares[tp] = row_total(hidden * hidden, 3)

    def square_copy(p):
        return copy_to(squares.at[tp], squares.at[tp], s_sq.at[p], r_sq.at[tp], {"tp": p})

    for d in range(1, tp_count):
        square_copy(lax.rem(tp + d, tp_count)).start()
    total = squares[tp]
    for d in range(1, tp_count):
        p = lax.rem(tp + d, tp_count)
        copy_to(squares.at[p], squares.at[p], s_sq.at[p], r_sq.at[p], {"tp": p}).wait_recv()
        total = total + squares[p]
    inverse = lax.rsqrt(total / model + 1e-06)
    first = jnp.where(lax.broadcasted_iota(jnp.int32, (8, 128), 0) == 0, 1.0, 0.0).astype(BF16)
    column = None
    for _ in range(3):
        piece = inverse.astype(BF16)
        inverse = inverse - piece.astype(F32)
        product = dot(piece, first, (0, 0))
        column = product if column is None else column + product
    normed = (hidden * column[:, :1] * gain_ref[:, mine]).astype(BF16)

    per = experts // sp_count * capacity
    places = lax.broadcasted_iota(jnp.int32, (rows, per), 1)

    def block_for(t):
        at = places + t * per
        chosen = (slots[0] == at)
        for s in slots[1:]:
            chosen = chosen | (s == at)
        return dot(jnp.where(chosen, 1.0, 0.0).astype(BF16), normed, (0, 0)).astype(BF16)

    def out_copy(t):
        return copy_to(
            outgoing.at[t], rows_ref.at[sp, :, mine], s_out.at[t], r_out.at[sp], {"sp": t}
        )

    def give(d, carry):
        t = lax.rem(sp + d, sp_count)
        outgoing[t] = block_for(t)
        out_copy(t).start()
        return carry

    lax.fori_loop(1, sp_count, give, 0)
    rows_ref[sp, :, mine] = block_for(sp)

    def own_copy(p, s):
        here = rows_ref.at[s, :, mine]
        return copy_to(here, here, s_own.at[p, s], r_col.at[tp, s], {"tp": p})

    def forward(o, s):
        here = rows_ref.at[s, :, span(o, cols)]
        return copy_to(here, here, s_fwd.at[o, s], r_col.at[o, s], {"tp": sibling})

    def arrived(o, s):
        here = rows_ref.at[s, :, span(o, cols)]
        copy_to(here, here, s_fwd.at[o, s], r_col.at[o, s], {"tp": sibling}).wait_recv()

    def peers():
        return [lax.rem(group + g, groups) * 2 + core for g in range(1, groups)]

    lag = 2

    def relay(d, carry):
        @pl.when(d < sp_count)
        def _():
            s = lax.rem(sp - d + sp_count, sp_count)

            @pl.when(d > 0)
            def _():
                here = rows_ref.at[s, :, mine]
                copy_to(here, here, s_out.at[s], r_out.at[s], {"sp": s}).wait_recv()

            for p in peers():
                own_copy(p, s).start()
            own_copy(sibling, s).start()

        @pl.when(d >= lag)
        def _():
            s = lax.rem(sp - (d - lag) + sp_count, sp_count)
            for o in peers():
                arrived(o, s)
                forward(o, s).start()

        return carry

    lax.fori_loop(0, sp_count + lag, relay, 0)

    def settle(s, carry):
        arrived(sibling, s)
        for g in range(1, groups):
            arrived(lax.rem(group + g, groups) * 2 + 1 - core, s)
        own_copy(sibling, s).wait_send()
        for p in peers():
            own_copy(p, s).wait_send()
            forward(p, s).wait_send()
        return carry

    lax.fori_loop(0, sp_count, settle, 0)

    def sent(d, carry):
        out_copy(lax.rem(sp + d, sp_count)).wait_send()
        return carry

    lax.fori_loop(1, sp_count, sent, 0)
    for d in range(1, tp_count):
        p = lax.rem(tp + d, tp_count)
        part_copy(p).wait_send()
        square_copy(p).wait_send()


def return_kernel(
    sp_count, tp_count,
    y_ref, hidden_ref, slot_ref, weight_ref,
    out_ref,
    from_sib, pair, from_peer, summed, back,
    s_sib, r_sib, s_peer, r_peer, s_back, r_back, s_own, s_fwd, r_col,
):
    sp, tp = lax.axis_index("sp"), lax.axis_index("tp")
    per, model = y_ref.shape[1:]
    rows = hidden_ref.shape[0]
    cols = model // tp_count
    mine = span(tp, cols)
    groups = tp_count // 2
    core, group = lax.rem(tp, 2), tp // 2
    sibling = group * 2 + 1 - core
    greet(sp_count, tp_count, sp, tp)

    def sib_copy(s, g):
        return copy_to(
            y_ref.at[s, :, span(g * 2 + 1 - core, cols)],
            from_sib.at[s, g],
            s_sib.at[s, g],
            r_sib.at[s, g],
            {"tp": sibling},
        )

    def peer_copy(s, g):
        return copy_to(
            pair.at[s, g],
            from_peer.at[s, group],
            s_peer.at[s, g],
            r_peer.at[s, group],
            {"tp": g * 2 + core},
        )

    def back_copy(t):
        return copy_to(summed.at[t], back.at[sp], s_back.at[t], r_back.at[sp], {"sp": t})

    def others():
        return [lax.rem(group + d, groups) for d in range(1, groups)]

    def order(d):
        return lax.rem(sp + 1 + d, sp_count)

    def open_up(d, carry):
        s = order(d)
        for g in others():
            sib_copy(s, g).start()
        sib_copy(s, group).start()
        return carry

    lax.fori_loop(0, sp_count, open_up, 0)
    lag = 2

    def step(d, carry):
        @pl.when(d < sp_count)
        def _():
            s = order(d)
            for g in others():
                sib_copy(s, g).wait_recv()
                pair[s, g] = (
                    y_ref[s, :, span(g * 2 + core, cols)].astype(F32) + from_sib[s, g].astype(F32)
                ).astype(BF16)
                peer_copy(s, g).start()
            sib_copy(s, group).wait_recv()

        @pl.when(d >= lag)
        def _():
            s = order(d - lag)
            total = y_ref[s, :, mine].astype(F32) + from_sib[s, group].astype(F32)
            for g in others():
                copy_to(
                    from_peer.at[s, g],
                    from_peer.at[s, g],
                    s_peer.at[s, g],
                    r_peer.at[s, g],
                    {"tp": g * 2 + core},
                ).wait_recv()
                total = total + from_peer[s, g].astype(F32)

            @pl.when(s != sp)
            def _():
                summed[s] = total.astype(BF16)
                back_copy(s).start()

            @pl.when(s == sp)
            def _():
                back[s] = total.astype(BF16)

        return carry

    lax.fori_loop(0, sp_count + lag, step, 0)
    slots = slot_ref[...]
    weights = weight_ref[...]
    places = lax.broadcasted_iota(jnp.int32, (rows, sp_count * per), 1)
    top = slots.shape[1]
    chosen = [jnp.where(slots[:, k : k + 1] == places, 1.0, 0.0).astype(BF16) for k in range(top)]

    def landed(d, carry):
        s = lax.rem(sp + d, sp_count)
        copy_to(back.at[s], back.at[s], s_back.at[s], r_back.at[s], {"sp": s}).wait_recv()
        return carry

    lax.fori_loop(1, sp_count, landed, 0)
    returned = back[...].reshape(sp_count * per, cols)
    result = hidden_ref[...] + sum(
        weights[:, k : k + 1] * dot(chosen[k], returned) for k in range(top)
    )
    out_ref[:, mine] = result.astype(BF16)

    def own_copy(p):
        here = out_ref.at[:, mine]
        return copy_to(here, here, s_own.at[p], r_col.at[tp], {"tp": p})

    def forward(o):
        here = out_ref.at[:, span(o, cols)]
        return copy_to(here, here, s_fwd.at[o], r_col.at[o], {"tp": sibling})

    peers = [g * 2 + core for g in others()]
    for p in peers:
        own_copy(p).start()
    own_copy(sibling).start()
    for p in peers:
        forward(p).wait_recv()
        forward(p).start()
    forward(sibling).wait_recv()
    for g in others():
        forward(g * 2 + 1 - core).wait_recv()
    own_copy(sibling).wait_send()
    for p in peers:
        own_copy(p).wait_send()
        forward(p).wait_send()

    def close(s, carry):
        sib_copy(s, group).wait_send()
        for g in others():
            sib_copy(s, g).wait_send()
            peer_copy(s, g).wait_send()
        return carry

    lax.fori_loop(0, sp_count, close, 0)

    def sent(d, carry):
        back_copy(lax.rem(sp + d, sp_count)).wait_send()
        return carry

    lax.fori_loop(1, sp_count, sent, 0)


def body(
    readout_query_vectors,
    attention_key_vectors,
    attention_content_vectors,
    step_size_preactivation,
    forgetting_preactivation,
    extra_forgetting_bias,
    subspace_normalizer_gain,
    skip_connection_stream,
    blender_projection_matrix,
    specialist_prenormal_gain,
    cluster_router_chance,
    specialist_chance_within_cluster,
    chosen_specialist_ids,
    specialist_switch_matrix,
    specialist_expansion_matrix,
    specialist_contraction_matrix,
):
    partial_branch = mixer_branch(
        readout_query_vectors,
        attention_key_vectors,
        attention_content_vectors,
        step_size_preactivation,
        forgetting_preactivation,
        extra_forgetting_bias,
        subspace_normalizer_gain,
        blender_projection_matrix,
    )
    tok_rows, model_width = skip_connection_stream.shape
    sp_count, tp_count = lax.axis_size("sp"), lax.axis_size("tp")
    local_experts = specialist_switch_matrix.shape[0]
    experts = local_experts * sp_count
    top_count = chosen_specialist_ids.shape[1]
    capacity = 2 * tok_rows * top_count // experts
    cols = model_width // tp_count
    per = local_experts * capacity
    groups = tp_count // 2
    vmem = pl.BlockSpec(memory_space=pltpu.VMEM)
    sems = pltpu.SemaphoreType.DMA
    hidden_cols, slots, rows_in = pl.pallas_call(
        functools.partial(route_kernel, sp_count, tp_count, experts, capacity),
        out_shape=[
            jax.ShapeDtypeStruct((tok_rows, cols), F32),
            jax.ShapeDtypeStruct((tok_rows, top_count), jnp.int32),
            jax.ShapeDtypeStruct((sp_count, per, model_width), BF16),
        ],
        in_specs=[vmem] * 4,
        out_specs=[vmem] * 3,
        scratch_shapes=[
            pltpu.VMEM((tp_count, tok_rows, cols), BF16),
            pltpu.VMEM((tp_count, 8, tok_rows), F32),
            pltpu.VMEM((sp_count, per, cols), BF16),
            sems((tp_count,)),
            sems((tp_count,)),
            sems((tp_count,)),
            sems((tp_count,)),
            sems((sp_count,)),
            sems((sp_count,)),
            sems((tp_count, sp_count)),
            sems((tp_count, sp_count)),
            sems((tp_count, sp_count)),
        ],
        compiler_params=pltpu.CompilerParams(
            collective_id=2, has_side_effects=True, vmem_limit_bytes=40 * 1024 * 1024
        ),
    )(
        partial_branch,
        skip_connection_stream,
        specialist_prenormal_gain.reshape(1, model_width),
        chosen_specialist_ids,
    )
    route_weight = (
        cluster_router_chance[:, None]
        * specialist_chance_within_cluster
        / jnp.sum(specialist_chance_within_cluster, axis=1, keepdims=True)
    )
    grouped = rows_in.reshape(sp_count, local_experts, capacity, model_width)
    gate_act = jnp.einsum(
        "secd,edf->secf", grouped, specialist_switch_matrix, preferred_element_type=jnp.float32
    )
    upward = jnp.einsum(
        "secd,edf->secf", grouped, specialist_expansion_matrix, preferred_element_type=jnp.float32
    )
    hidden = (jax.nn.silu(gate_act) * upward).astype(jnp.bfloat16)
    partial_value = jnp.einsum(
        "secf,efd->secd", hidden, specialist_contraction_matrix, preferred_element_type=jnp.float32
    )
    partial_value = partial_value.astype(jnp.bfloat16).reshape(rows_in.shape)
    return pl.pallas_call(
        functools.partial(return_kernel, sp_count, tp_count),
        out_shape=jax.ShapeDtypeStruct((tok_rows, model_width), BF16),
        in_specs=[vmem] * 4,
        out_specs=vmem,
        scratch_shapes=[
            pltpu.VMEM((sp_count, groups, per, cols), BF16),
            pltpu.VMEM((sp_count, groups, per, cols), BF16),
            pltpu.VMEM((sp_count, groups, per, cols), BF16),
            pltpu.VMEM((sp_count, per, cols), BF16),
            pltpu.VMEM((sp_count, per, cols), BF16),
            sems((sp_count, groups)),
            sems((sp_count, groups)),
            sems((sp_count, groups)),
            sems((sp_count, groups)),
            sems((sp_count,)),
            sems((sp_count,)),
            sems((tp_count,)),
            sems((tp_count,)),
            sems((tp_count,)),
        ],
        compiler_params=pltpu.CompilerParams(
            collective_id=3, has_side_effects=True, vmem_limit_bytes=50 * 1024 * 1024
        ),
    )(partial_value, hidden_cols, slots, route_weight)


def solution(mesh):
    in_specs = (
        P("sp", "tp"),
        P("sp", "tp"),
        P("sp", "tp"),
        P("sp", "tp"),
        P("sp", "tp"),
        P("sp", "tp"),
        P("tp"),
        P("sp", None),
        P("tp", None),
        P(),
        P("sp"),
        P("sp", None),
        P("sp", None),
        P("sp", None, "tp"),
        P("sp", None, "tp"),
        P("sp", "tp", None),
    )
    out_specs = P("sp", None)
    return jax.shard_map(body, mesh=mesh, in_specs=in_specs, out_specs=out_specs, check_vma=False)
```

```python
import functools
import math

import jax
import jax.numpy as jnp
from jax import lax
from jax.experimental import pallas as pl
from jax.experimental.pallas import tpu as pltpu
from jax.sharding import PartitionSpec as P

MESH = pl.DeviceIdType.MESH
F32 = jnp.float32
BF16 = jnp.bfloat16


def dot(left, right, axes=(1, 0)):
    return lax.dot_general(
        left, right, (((axes[0],), (axes[1],)), ((), ())), preferred_element_type=F32
    )


def halves(data):
    high = data.astype(BF16)
    return high, (data - high.astype(F32)).astype(BF16)


def dot3(left, right, axes=(1, 0)):
    lh, ll = halves(left)
    rh, rl = halves(right)
    return dot(lh, rh, axes) + (dot(lh, rl, axes) + dot(ll, rh, axes))


def dot1(left, right, axes=(1, 0)):
    return dot(left.astype(BF16), right.astype(BF16), axes)


def mixer_kernel(head_dim, segment, q_ref, k_ref, v_ref, a_ref, f_ref, b_ref, out_ref, map_ref, ka_ref):
    pair = pl.program_id(0)
    rows, width = q_ref.shape
    blocks = rows // segment
    per = width // head_dim
    shift = segment.bit_length() - 1
    row = lax.broadcasted_iota(jnp.int32, (rows, rows), 0)
    col = lax.broadcasted_iota(jnp.int32, (rows, rows), 1)
    same = (row >> shift) == (col >> shift)
    strict = same & (row > col)
    inclusive = same & (row >= col)
    triangle = jnp.where(inclusive, 1.0, 0.0).astype(BF16)
    lane = lax.broadcasted_iota(jnp.int32, (rows, width), 1)
    bias = b_ref[...]
    bias_lane = lax.broadcasted_iota(jnp.int32, bias.shape, 1)

    def spread(values):
        total = values[per - 1]
        for h in range(per - 2, -1, -1):
            total = jnp.where(lane < (h + 1) * head_dim, values[h], total)
        return total

    own_bias = [
        jnp.sum(jnp.where(bias_lane == pair * per + h, bias, 0.0), axis=1, keepdims=True)
        for h in range(per)
    ]
    decay = -(0.6065306597126334 / (1.0 + jnp.exp(-f_ref[...]))) + spread(own_bias)
    high, low = halves(decay)
    lowest = (decay - high.astype(F32) - low.astype(F32)).astype(BF16)
    cumulative = dot(triangle, high) + (dot(triangle, low) + dot(triangle, lowest))
    closing_rows = cumulative.reshape(blocks, segment, width)[:, segment - 1 :, :]
    closing = jnp.broadcast_to(closing_rows, (blocks, segment, width)).reshape(rows, width)
    keys = k_ref[...].astype(F32)
    squares = keys * keys
    norms = spread(
        [
            jnp.sum(squares[:, h * head_dim : (h + 1) * head_dim], axis=1, keepdims=True)
            for h in range(per)
        ]
    )
    removal = keys * lax.rsqrt(norms + 1e-06)
    rate = 1.0 / (1.0 + jnp.exp(-a_ref[...].astype(F32)))
    beta = removal * rate
    grow = jnp.exp(-cumulative)
    fade = jnp.exp(closing - cumulative)
    alpha_all = -removal * jnp.exp(cumulative - decay)
    beta_hat_all = beta * grow
    key_hat_all = keys * grow
    query_all = q_ref[...].astype(F32) * jnp.exp(cumulative)
    beta_bar_all = beta * fade
    key_bar_all = keys * fade
    values_all = v_ref[...]
    keep_all = jnp.exp(closing_rows)
    eye = lax.broadcasted_iota(jnp.int32, (head_dim, head_dim), 0) == lax.broadcasted_iota(
        jnp.int32, (head_dim, head_dim), 1
    )
    outs, maps = [], []
    for h in range(per):
        part = slice(h * head_dim, (h + 1) * head_dim)
        alpha, beta_hat, key_hat = alpha_all[:, part], beta_hat_all[:, part], key_hat_all[:, part]
        query, values = query_all[:, part], values_all[:, part]
        beta_bar, key_bar = beta_bar_all[:, part], key_bar_all[:, part]
        lower = jnp.where(strict, dot3(alpha, beta_hat, (1, 1)), 0.0)
        remove_write = jnp.where(strict, dot1(alpha, key_hat, (1, 1)), 0.0)
        read_remove = jnp.where(inclusive, dot1(query, beta_hat, (1, 1)), 0.0)
        read_write = jnp.where(inclusive, dot1(query, key_hat, (1, 1)), 0.0)
        lh, ll = halves(lower)
        inverse = jnp.where(row == col, 1.0, jnp.where((row >> 1) == (col >> 1), lower, 0.0))
        for s in range(1, shift):
            off = ((row >> (s + 1)) == (col >> (s + 1))) & ((row >> s) != (col >> s))
            near = inverse.astype(BF16)
            reach = dot(jnp.where(off, lower, 0.0).astype(BF16), near)
            inverse = inverse + dot(near, reach.astype(BF16))
        wh, wl = halves(remove_write)
        side = jnp.concatenate([alpha, dot(wh, values) + dot(wl, values)], axis=1)
        near = inverse.astype(BF16)
        solved = dot(near, side.astype(BF16))
        sh, sl = halves(solved)
        miss = side - solved + (dot(lh, sh) + (dot(lh, sl) + dot(ll, sh)))
        solved = solved + dot(near, miss.astype(BF16))
        read = dot1(read_remove, solved)
        read_map = query + read[:, :head_dim]
        local = read[:, head_dim:] + dot(read_write.astype(BF16), values)
        state = jnp.concatenate(
            [jnp.where(eye, 1.0, 0.0), jnp.zeros((head_dim, head_dim), F32)], axis=0
        )
        out_rows, map_rows = [], []
        for b in range(blocks):
            at = slice(b * segment, (b + 1) * segment)
            seen = dot1(read_map[at], state, (1, 1))
            map_rows.append(seen[:, :head_dim])
            out_rows.append(local[at] + seen[:, head_dim:])
            step = dot3(solved[at], beta_bar[at], (0, 0))
            bh, bl = halves(key_bar[at])
            add = step[head_dim:] + dot(values[at], bh, (0, 0)) + dot(values[at], bl, (0, 0))
            keep = step[:head_dim] + jnp.where(eye, keep_all[b][:, part], 0.0)
            state = dot3(state, keep)
            state = jnp.concatenate([state[:head_dim], state[head_dim:] + add], axis=0)
        outs.append(jnp.concatenate(out_rows, axis=0))
        maps.append(jnp.concatenate(map_rows, axis=0))
        ka_ref[h] = jnp.concatenate([state[:head_dim], state[head_dim:]], axis=1).astype(BF16)
    out_ref[...] = jnp.concatenate(outs, axis=1)
    map_ref[...] = jnp.concatenate(maps, axis=1).astype(BF16)


def exchange_kernel(count, per, workers, ka_ref, st_ref, got, fold, send1, recv1, send2, recv2):
    me = lax.axis_index("sp")
    dim = ka_ref.shape[1]
    barrier = pltpu.get_barrier_semaphore()
    for d in range(1, count):
        pl.semaphore_signal(
            barrier, inc=1, device_id={"sp": lax.rem(me + d, count)}, device_id_type=MESH
        )
    pl.semaphore_wait(barrier, count - 1)

    def first(t, owner):
        return pltpu.make_async_remote_copy(
            src_ref=ka_ref.at[pl.ds(t * per, per)],
            dst_ref=got.at[owner],
            send_sem=send1.at[t],
            recv_sem=recv1.at[owner],
            device_id={"sp": t},
            device_id_type=MESH,
        )

    def second(t, owner):
        return pltpu.make_async_remote_copy(
            src_ref=fold.at[t],
            dst_ref=st_ref.at[pl.ds(owner * per, per)],
            send_sem=send2.at[t],
            recv_sem=recv2.at[owner],
            device_id={"sp": t},
            device_id_type=MESH,
        )

    for t in range(workers):
        @pl.when(t != me)
        def _(t=t):
            first(t, me).start()

    def work():
        got[me] = ka_ref[pl.ds(me * per, per)]
        state = [jnp.zeros((dim, dim), F32) for _ in range(per)]
        for j in range(count):
            @pl.when(j != me)
            def _(j=j):
                pltpu.make_async_remote_copy(
                    src_ref=got.at[j],
                    dst_ref=got.at[j],
                    send_sem=send1.at[0],
                    recv_sem=recv1.at[j],
                    device_id={"sp": j},
                    device_id_type=MESH,
                ).wait_recv()
            for i in range(per):
                fold[j, i] = jnp.concatenate([state[i], jnp.zeros_like(state[i])], axis=1).astype(BF16)
                both = got[j, i]
                keep, add = both[:, :dim], both[:, dim:].astype(F32)
                sh, sl = halves(state[i])
                state[i] = dot(sh, keep) + dot(sl, keep) + add
        for t in range(count):
            @pl.when(t != me)
            def _(t=t):
                second(t, me).start()
        st_ref[pl.ds(me * per, per)] = fold[me]
        for t in range(count):
            @pl.when(t != me)
            def _(t=t):
                second(t, me).wait_send()

    if workers == count:
        work()
    else:
        pl.when(me < workers)(work)
    for t in range(workers):
        @pl.when(t != me)
        def _(t=t):
            first(t, me).wait_send()
            pltpu.make_async_remote_copy(
                src_ref=fold.at[t],
                dst_ref=st_ref.at[pl.ds(t * per, per)],
                send_sem=send2.at[0],
                recv_sem=recv2.at[t],
                device_id={"sp": t},
                device_id_type=MESH,
            ).wait_recv()


def finish_kernel(head_dim, out_ref, map_ref, st_ref, gain_ref, w_ref, part_ref, mixed):
    @pl.when(pl.program_id(0) == 0)
    def _():
        for h in range(out_ref.shape[1] // head_dim):
            part = slice(h * head_dim, (h + 1) * head_dim)
            states = st_ref[h][:, :head_dim]
            output = out_ref[:, part] + dot(map_ref[:, part], states, (1, 1))
            centered = output - jnp.mean(output, axis=1, keepdims=True)
            spread = jnp.mean(centered * centered, axis=1, keepdims=True)
            mixed[:, part] = (centered * lax.rsqrt(spread + 0.00064) * gain_ref[:, part]).astype(BF16)

    part_ref[...] = dot(mixed[...], w_ref[...]).astype(BF16)


def mixer_branch(query, key, value, step, forget, bias, gain, blender):
    count = lax.axis_size("sp")
    rows, channels = query.shape
    heads = bias.shape[1]
    head_dim = channels // heads
    segment = min(64, rows)
    width = 2 * head_dim
    pairs = heads // 2
    block = pl.BlockSpec((rows, width), lambda p: (0, p))
    out, maps, ka = pl.pallas_call(
        functools.partial(mixer_kernel, head_dim, segment),
        grid=(pairs,),
        in_specs=[block] * 5 + [pl.BlockSpec((rows, heads), lambda p: (0, 0))],
        out_specs=[block, block, pl.BlockSpec((2, head_dim, width), lambda p: (p, 0, 0))],
        out_shape=[
            jax.ShapeDtypeStruct((rows, channels), F32),
            jax.ShapeDtypeStruct((rows, channels), BF16),
            jax.ShapeDtypeStruct((heads, head_dim, width), BF16),
        ],
        compiler_params=pltpu.CompilerParams(vmem_limit_bytes=50 * 1024 * 1024),
    )(query, key, value, step, forget, bias)
    per = max(1, heads // count)
    workers = heads // per
    vmem = pl.BlockSpec(memory_space=pltpu.VMEM)
    states = pl.pallas_call(
        functools.partial(exchange_kernel, count, per, workers),
        out_shape=jax.ShapeDtypeStruct((heads, head_dim, width), BF16),
        in_specs=[vmem],
        out_specs=vmem,
        scratch_shapes=[
            pltpu.VMEM((count, per, head_dim, width), BF16),
            pltpu.VMEM((count, per, head_dim, width), BF16),
            pltpu.SemaphoreType.DMA((count,)),
            pltpu.SemaphoreType.DMA((count,)),
            pltpu.SemaphoreType.DMA((count,)),
            pltpu.SemaphoreType.DMA((count,)),
        ],
        compiler_params=pltpu.CompilerParams(collective_id=1, has_side_effects=True),
    )(ka)
    model_width = blender.shape[1]
    tile = min(512, model_width)
    whole = lambda *shape: pl.BlockSpec(shape, lambda p: (0,) * len(shape))
    return pl.pallas_call(
        functools.partial(finish_kernel, head_dim),
        grid=(model_width // tile,),
        in_specs=[
            whole(rows, channels),
            whole(rows, channels),
            whole(heads, head_dim, width),
            whole(1, channels),
            pl.BlockSpec((channels, tile), lambda p: (0, p)),
        ],
        out_specs=pl.BlockSpec((rows, tile), lambda p: (0, p)),
        out_shape=jax.ShapeDtypeStruct((rows, model_width), BF16),
        scratch_shapes=[pltpu.VMEM((rows, channels), BF16)],
    )(out, maps, states, gain.reshape(1, channels), blender)


def greet(sp_count, tp_count, sp, tp):
    barrier = pltpu.get_barrier_semaphore()
    for d in range(1, sp_count):
        pl.semaphore_signal(
            barrier, inc=1, device_id={"sp": lax.rem(sp + d, sp_count)}, device_id_type=MESH
        )
    for d in range(1, tp_count):
        pl.semaphore_signal(
            barrier, inc=1, device_id={"tp": lax.rem(tp + d, tp_count)}, device_id_type=MESH
        )
    pl.semaphore_wait(barrier, sp_count + tp_count - 2)


def copy_to(src, dst, send, recv, device):
    return pltpu.make_async_remote_copy(
        src_ref=src,
        dst_ref=dst,
        send_sem=send,
        recv_sem=recv,
        device_id=device,
        device_id_type=MESH,
    )


def span(index, size):
    return pl.ds(pl.multiple_of(index * size, size), size)


def row_total(data, terms):
    ones = jnp.ones((8, data.shape[1]), BF16)
    total = None
    for _ in range(terms):
        piece = data.astype(BF16)
        data = data - piece.astype(F32)
        product = dot(ones, piece, (1, 1))
        total = product if total is None else total + product
    return total


def route_kernel(
    sp_count, tp_count, experts, capacity,
    part_ref, skip_ref, gain_ref, ids_ref,
    hidden_ref, slot_ref, rows_ref,
    gathered, squares, outgoing,
    s_part, r_part, s_sq, r_sq, s_out, r_out, s_own, s_fwd, r_col,
):
    sp, tp = lax.axis_index("sp"), lax.axis_index("tp")
    rows, model = part_ref.shape
    cols = model // tp_count
    mine = span(tp, cols)
    groups = tp_count // 2
    core, group = lax.rem(tp, 2), tp // 2
    sibling = group * 2 + 1 - core
    greet(sp_count, tp_count, sp, tp)

    def part_copy(p):
        return copy_to(
            part_ref.at[:, span(p, cols)], gathered.at[tp], s_part.at[p], r_part.at[tp], {"tp": p}
        )

    for d in range(1, tp_count):
        part_copy(lax.rem(tp + d, tp_count)).start()

    ids = ids_ref[...]
    top = ids.shape[1]
    lanes = lax.broadcasted_iota(jnp.int32, (rows, experts), 1)
    named = [ids[:, k : k + 1] == lanes for k in range(top)]
    anyone = sum(jnp.where(n, 1.0, 0.0) for n in named).astype(BF16)
    r0 = lax.broadcasted_iota(jnp.int32, (rows, rows), 0)
    r1 = lax.broadcasted_iota(jnp.int32, (rows, rows), 1)
    before = dot(jnp.where(r0 > r1, 1.0, 0.0).astype(BF16), anyone)
    slots = [
        jnp.sum(
            jnp.where(n, before + lanes.astype(F32) * capacity, 0.0), axis=1, keepdims=True
        ).astype(jnp.int32)
        for n in named
    ]
    slot_ref[...] = jnp.concatenate(slots, axis=1)

    branch = part_ref[:, mine].astype(F32)
    for d in range(1, tp_count):
        p = lax.rem(tp + d, tp_count)
        copy_to(gathered.at[p], gathered.at[p], s_part.at[p], r_part.at[p], {"tp": p}).wait_recv()
        branch = branch + gathered[p].astype(F32)
    hidden = skip_ref[:, mine].astype(F32) + branch
    hidden_ref[...] = hidden
    squares[tp] = row_total(hidden * hidden, 3)

    def square_copy(p):
        return copy_to(squares.at[tp], squares.at[tp], s_sq.at[p], r_sq.at[tp], {"tp": p})

    for d in range(1, tp_count):
        square_copy(lax.rem(tp + d, tp_count)).start()
    total = squares[tp]
    for d in range(1, tp_count):
        p = lax.rem(tp + d, tp_count)
        copy_to(squares.at[p], squares.at[p], s_sq.at[p], r_sq.at[p], {"tp": p}).wait_recv()
        total = total + squares[p]
    inverse = lax.rsqrt(total / model + 1e-06)
    first = jnp.where(lax.broadcasted_iota(jnp.int32, (8, 128), 0) == 0, 1.0, 0.0).astype(BF16)
    column = None
    for _ in range(3):
        piece = inverse.astype(BF16)
        inverse = inverse - piece.astype(F32)
        product = dot(piece, first, (0, 0))
        column = product if column is None else column + product
    normed = (hidden * column[:, :1] * gain_ref[:, mine]).astype(BF16)

    per = experts // sp_count * capacity
    places = lax.broadcasted_iota(jnp.int32, (rows, per), 1)

    def block_for(t):
        at = places + t * per
        chosen = (slots[0] == at)
        for s in slots[1:]:
            chosen = chosen | (s == at)
        return dot(jnp.where(chosen, 1.0, 0.0).astype(BF16), normed, (0, 0)).astype(BF16)

    def out_copy(t):
        return copy_to(
            outgoing.at[t], rows_ref.at[sp, :, mine], s_out.at[t], r_out.at[sp], {"sp": t}
        )

    def give(d, carry):
        t = lax.rem(sp + d, sp_count)
        outgoing[t] = block_for(t)
        out_copy(t).start()
        return carry

    lax.fori_loop(1, sp_count, give, 0)
    rows_ref[sp, :, mine] = block_for(sp)

    def own_copy(p, s):
        here = rows_ref.at[s, :, mine]
        return copy_to(here, here, s_own.at[p, s], r_col.at[tp, s], {"tp": p})

    def forward(o, s):
        here = rows_ref.at[s, :, span(o, cols)]
        return copy_to(here, here, s_fwd.at[o, s], r_col.at[o, s], {"tp": sibling})

    def arrived(o, s):
        here = rows_ref.at[s, :, span(o, cols)]
        copy_to(here, here, s_fwd.at[o, s], r_col.at[o, s], {"tp": sibling}).wait_recv()

    def peers():
        return [lax.rem(group + g, groups) * 2 + core for g in range(1, groups)]

    lag = 2

    def relay(d, carry):
        @pl.when(d < sp_count)
        def _():
            s = lax.rem(sp - d + sp_count, sp_count)

            @pl.when(d > 0)
            def _():
                here = rows_ref.at[s, :, mine]
                copy_to(here, here, s_out.at[s], r_out.at[s], {"sp": s}).wait_recv()

            for p in peers():
                own_copy(p, s).start()
            own_copy(sibling, s).start()

        @pl.when(d >= lag)
        def _():
            s = lax.rem(sp - (d - lag) + sp_count, sp_count)
            for o in peers():
                arrived(o, s)
                forward(o, s).start()

        return carry

    lax.fori_loop(0, sp_count + lag, relay, 0)

    def settle(s, carry):
        arrived(sibling, s)
        for g in range(1, groups):
            arrived(lax.rem(group + g, groups) * 2 + 1 - core, s)
        own_copy(sibling, s).wait_send()
        for p in peers():
            own_copy(p, s).wait_send()
            forward(p, s).wait_send()
        return carry

    lax.fori_loop(0, sp_count, settle, 0)

    def sent(d, carry):
        out_copy(lax.rem(sp + d, sp_count)).wait_send()
        return carry

    lax.fori_loop(1, sp_count, sent, 0)
    for d in range(1, tp_count):
        p = lax.rem(tp + d, tp_count)
        part_copy(p).wait_send()
        square_copy(p).wait_send()


def return_kernel(
    sp_count, tp_count,
    rows_ref, switch_ref, expand_ref, contract_ref, hidden_ref, slot_ref, weight_ref,
    out_ref,
    y_ref, from_sib, pair, from_peer, summed, back,
    s_sib, r_sib, s_peer, r_peer, s_back, r_back, s_own, s_fwd, r_col,
):
    sp, tp = lax.axis_index("sp"), lax.axis_index("tp")
    per, model = y_ref.shape[1:]
    rows = hidden_ref.shape[0]
    cols = model // tp_count
    mine = span(tp, cols)
    groups = tp_count // 2
    core, group = lax.rem(tp, 2), tp // 2
    sibling = group * 2 + 1 - core
    greet(sp_count, tp_count, sp, tp)

    def sib_copy(s, g):
        return copy_to(
            y_ref.at[s, :, span(g * 2 + 1 - core, cols)],
            from_sib.at[s, g],
            s_sib.at[s, g],
            r_sib.at[s, g],
            {"tp": sibling},
        )

    def peer_copy(s, g):
        return copy_to(
            pair.at[s, g],
            from_peer.at[s, group],
            s_peer.at[s, g],
            r_peer.at[s, group],
            {"tp": g * 2 + core},
        )

    def back_copy(t):
        return copy_to(summed.at[t], back.at[sp], s_back.at[t], r_back.at[sp], {"sp": t})

    def others():
        return [lax.rem(group + d, groups) for d in range(1, groups)]

    def order(d):
        return lax.rem(sp + 1 + d, sp_count)

    local = switch_ref.shape[0]
    capacity = per // local
    chunk = math.gcd(sp_count, max(1, 256 // capacity))
    chunks = sp_count // chunk

    def expert(i):
        at = [order(i * chunk + c) for c in range(chunk)]
        for e in range(local):
            inside = slice(e * capacity, (e + 1) * capacity)
            data = jnp.concatenate([rows_ref[s, inside, :] for s in at], axis=0)
            gate = dot(data, switch_ref[e])
            units = (gate / (1.0 + jnp.exp(-gate)) * dot(data, expand_ref[e])).astype(BF16)
            value = dot(units, contract_ref[e]).astype(BF16)
            for c in range(chunk):
                y_ref[at[c], inside, :] = value[c * capacity : (c + 1) * capacity]
        for s in at:
            for g in others():
                sib_copy(s, g).start()
            sib_copy(s, group).start()

    def meet(s):
        for g in others():
            sib_copy(s, g).wait_recv()
            pair[s, g] = (
                y_ref[s, :, span(g * 2 + core, cols)].astype(F32) + from_sib[s, g].astype(F32)
            ).astype(BF16)
            peer_copy(s, g).start()
        sib_copy(s, group).wait_recv()

    def total_up(s):
        total = y_ref[s, :, mine].astype(F32) + from_sib[s, group].astype(F32)
        for g in others():
            copy_to(
                from_peer.at[s, g],
                from_peer.at[s, g],
                s_peer.at[s, g],
                r_peer.at[s, g],
                {"tp": g * 2 + core},
            ).wait_recv()
            total = total + from_peer[s, g].astype(F32)

        @pl.when(s != sp)
        def _():
            summed[s] = total.astype(BF16)
            back_copy(s).start()

        @pl.when(s == sp)
        def _():
            back[s] = total.astype(BF16)

    def step(i, carry):
        @pl.when(i < chunks)
        def _():
            expert(i)

        @pl.when((i >= 1) & (i <= chunks))
        def _():
            for c in range(chunk):
                meet(order((i - 1) * chunk + c))

        @pl.when(i >= 2)
        def _():
            for c in range(chunk):
                total_up(order((i - 2) * chunk + c))

        return carry

    lax.fori_loop(0, chunks + 2, step, 0)
    slots = slot_ref[...]
    weights = weight_ref[...]
    places = lax.broadcasted_iota(jnp.int32, (rows, sp_count * per), 1)
    top = slots.shape[1]
    chosen = [jnp.where(slots[:, k : k + 1] == places, 1.0, 0.0).astype(BF16) for k in range(top)]

    def landed(d, carry):
        s = lax.rem(sp + d, sp_count)
        copy_to(back.at[s], back.at[s], s_back.at[s], r_back.at[s], {"sp": s}).wait_recv()
        return carry

    lax.fori_loop(1, sp_count, landed, 0)
    returned = back[...].reshape(sp_count * per, cols)
    result = hidden_ref[...] + sum(
        weights[:, k : k + 1] * dot(chosen[k], returned) for k in range(top)
    )
    out_ref[:, mine] = result.astype(BF16)

    def own_copy(p):
        here = out_ref.at[:, mine]
        return copy_to(here, here, s_own.at[p], r_col.at[tp], {"tp": p})

    def forward(o):
        here = out_ref.at[:, span(o, cols)]
        return copy_to(here, here, s_fwd.at[o], r_col.at[o], {"tp": sibling})

    peers = [g * 2 + core for g in others()]
    for p in peers:
        own_copy(p).start()
    own_copy(sibling).start()
    for p in peers:
        forward(p).wait_recv()
        forward(p).start()
    forward(sibling).wait_recv()
    for g in others():
        forward(g * 2 + 1 - core).wait_recv()
    own_copy(sibling).wait_send()
    for p in peers:
        own_copy(p).wait_send()
        forward(p).wait_send()

    def close(s, carry):
        sib_copy(s, group).wait_send()
        for g in others():
            sib_copy(s, g).wait_send()
            peer_copy(s, g).wait_send()
        return carry

    lax.fori_loop(0, sp_count, close, 0)

    def sent(d, carry):
        back_copy(lax.rem(sp + d, sp_count)).wait_send()
        return carry

    lax.fori_loop(1, sp_count, sent, 0)


def body(
    readout_query_vectors,
    attention_key_vectors,
    attention_content_vectors,
    step_size_preactivation,
    forgetting_preactivation,
    extra_forgetting_bias,
    subspace_normalizer_gain,
    skip_connection_stream,
    blender_projection_matrix,
    specialist_prenormal_gain,
    cluster_router_chance,
    specialist_chance_within_cluster,
    chosen_specialist_ids,
    specialist_switch_matrix,
    specialist_expansion_matrix,
    specialist_contraction_matrix,
):
    partial_branch = mixer_branch(
        readout_query_vectors,
        attention_key_vectors,
        attention_content_vectors,
        step_size_preactivation,
        forgetting_preactivation,
        extra_forgetting_bias,
        subspace_normalizer_gain,
        blender_projection_matrix,
    )
    tok_rows, model_width = skip_connection_stream.shape
    sp_count, tp_count = lax.axis_size("sp"), lax.axis_size("tp")
    local_experts = specialist_switch_matrix.shape[0]
    experts = local_experts * sp_count
    top_count = chosen_specialist_ids.shape[1]
    capacity = 2 * tok_rows * top_count // experts
    cols = model_width // tp_count
    per = local_experts * capacity
    groups = tp_count // 2
    vmem = pl.BlockSpec(memory_space=pltpu.VMEM)
    sems = pltpu.SemaphoreType.DMA
    hidden_cols, slots, rows_in = pl.pallas_call(
        functools.partial(route_kernel, sp_count, tp_count, experts, capacity),
        out_shape=[
            jax.ShapeDtypeStruct((tok_rows, cols), F32),
            jax.ShapeDtypeStruct((tok_rows, top_count), jnp.int32),
            jax.ShapeDtypeStruct((sp_count, per, model_width), BF16),
        ],
        in_specs=[vmem] * 4,
        out_specs=[vmem] * 3,
        scratch_shapes=[
            pltpu.VMEM((tp_count, tok_rows, cols), BF16),
            pltpu.VMEM((tp_count, 8, tok_rows), F32),
            pltpu.VMEM((sp_count, per, cols), BF16),
            sems((tp_count,)),
            sems((tp_count,)),
            sems((tp_count,)),
            sems((tp_count,)),
            sems((sp_count,)),
            sems((sp_count,)),
            sems((tp_count, sp_count)),
            sems((tp_count, sp_count)),
            sems((tp_count, sp_count)),
        ],
        compiler_params=pltpu.CompilerParams(
            collective_id=2, has_side_effects=True, vmem_limit_bytes=40 * 1024 * 1024
        ),
    )(
        partial_branch,
        skip_connection_stream,
        specialist_prenormal_gain.reshape(1, model_width),
        chosen_specialist_ids,
    )
    route_weight = (
        cluster_router_chance[:, None]
        * specialist_chance_within_cluster
        / jnp.sum(specialist_chance_within_cluster, axis=1, keepdims=True)
    )
    return pl.pallas_call(
        functools.partial(return_kernel, sp_count, tp_count),
        out_shape=jax.ShapeDtypeStruct((tok_rows, model_width), BF16),
        in_specs=[vmem] * 7,
        out_specs=vmem,
        scratch_shapes=[
            pltpu.VMEM((sp_count, per, model_width), BF16),
            pltpu.VMEM((sp_count, groups, per, cols), BF16),
            pltpu.VMEM((sp_count, groups, per, cols), BF16),
            pltpu.VMEM((sp_count, groups, per, cols), BF16),
            pltpu.VMEM((sp_count, per, cols), BF16),
            pltpu.VMEM((sp_count, per, cols), BF16),
            sems((sp_count, groups)),
            sems((sp_count, groups)),
            sems((sp_count, groups)),
            sems((sp_count, groups)),
            sems((sp_count,)),
            sems((sp_count,)),
            sems((tp_count,)),
            sems((tp_count,)),
            sems((tp_count,)),
        ],
        compiler_params=pltpu.CompilerParams(
            collective_id=3, has_side_effects=True, vmem_limit_bytes=50 * 1024 * 1024
        ),
    )(
        rows_in,
        specialist_switch_matrix,
        specialist_expansion_matrix,
        specialist_contraction_matrix,
        hidden_cols,
        slots,
        route_weight,
    )


def solution(mesh):
    in_specs = (
        P("sp", "tp"),
        P("sp", "tp"),
        P("sp", "tp"),
        P("sp", "tp"),
        P("sp", "tp"),
        P("sp", "tp"),
        P("tp"),
        P("sp", None),
        P("tp", None),
        P(),
        P("sp"),
        P("sp", None),
        P("sp", None),
        P("sp", None, "tp"),
        P("sp", None, "tp"),
        P("sp", "tp", None),
    )
    out_specs = P("sp", None)
    return jax.shard_map(body, mesh=mesh, in_specs=in_specs, out_specs=out_specs, check_vma=False)
```

```python
import functools
import math

import jax
import jax.numpy as jnp
from jax import lax
from jax.experimental import pallas as pl
from jax.experimental.pallas import tpu as pltpu
from jax.sharding import PartitionSpec as P

MESH = pl.DeviceIdType.MESH
F32 = jnp.float32
BF16 = jnp.bfloat16


def dot(left, right, axes=(1, 0)):
    return lax.dot_general(
        left, right, (((axes[0],), (axes[1],)), ((), ())), preferred_element_type=F32
    )


def halves(data):
    high = data.astype(BF16)
    return high, (data - high.astype(F32)).astype(BF16)


def dot3(left, right, axes=(1, 0)):
    lh, ll = halves(left)
    rh, rl = halves(right)
    return dot(lh, rh, axes) + (dot(lh, rl, axes) + dot(ll, rh, axes))


def dot1(left, right, axes=(1, 0)):
    return dot(left.astype(BF16), right.astype(BF16), axes)


def mixer_kernel(head_dim, segment, q_ref, k_ref, v_ref, a_ref, f_ref, b_ref, out_ref, map_ref, ka_ref):
    pair = pl.program_id(0)
    rows, width = q_ref.shape
    blocks = rows // segment
    per = width // head_dim
    shift = segment.bit_length() - 1
    row = lax.broadcasted_iota(jnp.int32, (rows, rows), 0)
    col = lax.broadcasted_iota(jnp.int32, (rows, rows), 1)
    same = (row >> shift) == (col >> shift)
    strict = same & (row > col)
    inclusive = same & (row >= col)
    triangle = jnp.where(inclusive, 1.0, 0.0).astype(BF16)
    lane = lax.broadcasted_iota(jnp.int32, (rows, width), 1)
    bias = b_ref[...]
    bias_lane = lax.broadcasted_iota(jnp.int32, bias.shape, 1)

    def spread(values):
        total = values[per - 1]
        for h in range(per - 2, -1, -1):
            total = jnp.where(lane < (h + 1) * head_dim, values[h], total)
        return total

    own_bias = [
        jnp.sum(jnp.where(bias_lane == pair * per + h, bias, 0.0), axis=1, keepdims=True)
        for h in range(per)
    ]
    decay = -(0.6065306597126334 / (1.0 + jnp.exp(-f_ref[...]))) + spread(own_bias)
    high, low = halves(decay)
    lowest = (decay - high.astype(F32) - low.astype(F32)).astype(BF16)
    cumulative = dot(triangle, high) + (dot(triangle, low) + dot(triangle, lowest))
    closing_rows = cumulative.reshape(blocks, segment, width)[:, segment - 1 :, :]
    closing = jnp.broadcast_to(closing_rows, (blocks, segment, width)).reshape(rows, width)
    keys = k_ref[...].astype(F32)
    squares = keys * keys
    norms = spread(
        [
            jnp.sum(squares[:, h * head_dim : (h + 1) * head_dim], axis=1, keepdims=True)
            for h in range(per)
        ]
    )
    removal = keys * lax.rsqrt(norms + 1e-06)
    rate = 1.0 / (1.0 + jnp.exp(-a_ref[...].astype(F32)))
    beta = removal * rate
    grow = jnp.exp(-cumulative)
    fade = jnp.exp(closing - cumulative)
    alpha_all = -removal * jnp.exp(cumulative - decay)
    beta_hat_all = beta * grow
    key_hat_all = keys * grow
    query_all = q_ref[...].astype(F32) * jnp.exp(cumulative)
    beta_bar_all = beta * fade
    key_bar_all = keys * fade
    values_all = v_ref[...]
    keep_all = jnp.exp(closing_rows)
    eye = lax.broadcasted_iota(jnp.int32, (head_dim, head_dim), 0) == lax.broadcasted_iota(
        jnp.int32, (head_dim, head_dim), 1
    )
    outs, maps = [], []
    for h in range(per):
        part = slice(h * head_dim, (h + 1) * head_dim)
        alpha, beta_hat, key_hat = alpha_all[:, part], beta_hat_all[:, part], key_hat_all[:, part]
        query, values = query_all[:, part], values_all[:, part]
        beta_bar, key_bar = beta_bar_all[:, part], key_bar_all[:, part]
        lower = jnp.where(strict, dot3(alpha, beta_hat, (1, 1)), 0.0)
        remove_write = jnp.where(strict, dot1(alpha, key_hat, (1, 1)), 0.0)
        read_remove = jnp.where(inclusive, dot1(query, beta_hat, (1, 1)), 0.0)
        read_write = jnp.where(inclusive, dot1(query, key_hat, (1, 1)), 0.0)
        lh, ll = halves(lower)
        inverse = jnp.where(row == col, 1.0, jnp.where((row >> 1) == (col >> 1), lower, 0.0))
        for s in range(1, shift):
            off = ((row >> (s + 1)) == (col >> (s + 1))) & ((row >> s) != (col >> s))
            near = inverse.astype(BF16)
            reach = dot(jnp.where(off, lower, 0.0).astype(BF16), near)
            inverse = inverse + dot(near, reach.astype(BF16))
        wh, wl = halves(remove_write)
        side = jnp.concatenate([alpha, dot(wh, values) + dot(wl, values)], axis=1)
        near = inverse.astype(BF16)
        solved = dot(near, side.astype(BF16))
        sh, sl = halves(solved)
        miss = side - solved + (dot(lh, sh) + (dot(lh, sl) + dot(ll, sh)))
        solved = solved + dot(near, miss.astype(BF16))
        read = dot1(read_remove, solved)
        read_map = query + read[:, :head_dim]
        local = read[:, head_dim:] + dot(read_write.astype(BF16), values)
        state = jnp.concatenate(
            [jnp.where(eye, 1.0, 0.0), jnp.zeros((head_dim, head_dim), F32)], axis=0
        )
        out_rows, map_rows = [], []
        for b in range(blocks):
            at = slice(b * segment, (b + 1) * segment)
            seen = dot1(read_map[at], state, (1, 1))
            map_rows.append(seen[:, :head_dim])
            out_rows.append(local[at] + seen[:, head_dim:])
            step = dot3(solved[at], beta_bar[at], (0, 0))
            bh, bl = halves(key_bar[at])
            add = step[head_dim:] + dot(values[at], bh, (0, 0)) + dot(values[at], bl, (0, 0))
            keep = step[:head_dim] + jnp.where(eye, keep_all[b][:, part], 0.0)
            state = dot3(state, keep)
            state = jnp.concatenate([state[:head_dim], state[head_dim:] + add], axis=0)
        outs.append(jnp.concatenate(out_rows, axis=0))
        maps.append(jnp.concatenate(map_rows, axis=0))
        ka_ref[h] = jnp.concatenate([state[:head_dim], state[head_dim:]], axis=1).astype(BF16)
    out_ref[...] = jnp.concatenate(outs, axis=1)
    map_ref[...] = jnp.concatenate(maps, axis=1).astype(BF16)


def exchange_kernel(count, per, workers, ka_ref, st_ref, got, fold, send1, recv1, send2, recv2):
    me = lax.axis_index("sp")
    dim = ka_ref.shape[1]
    barrier = pltpu.get_barrier_semaphore()
    for d in range(1, count):
        pl.semaphore_signal(
            barrier, inc=1, device_id={"sp": lax.rem(me + d, count)}, device_id_type=MESH
        )
    pl.semaphore_wait(barrier, count - 1)

    def first(t, owner):
        return pltpu.make_async_remote_copy(
            src_ref=ka_ref.at[pl.ds(t * per, per)],
            dst_ref=got.at[owner],
            send_sem=send1.at[t],
            recv_sem=recv1.at[owner],
            device_id={"sp": t},
            device_id_type=MESH,
        )

    def second(t, owner):
        return pltpu.make_async_remote_copy(
            src_ref=fold.at[t],
            dst_ref=st_ref.at[pl.ds(owner * per, per)],
            send_sem=send2.at[t],
            recv_sem=recv2.at[owner],
            device_id={"sp": t},
            device_id_type=MESH,
        )

    for t in range(workers):
        @pl.when(t != me)
        def _(t=t):
            first(t, me).start()

    def work():
        got[me] = ka_ref[pl.ds(me * per, per)]
        state = [jnp.zeros((dim, dim), F32) for _ in range(per)]
        for j in range(count):
            @pl.when(j != me)
            def _(j=j):
                pltpu.make_async_remote_copy(
                    src_ref=got.at[j],
                    dst_ref=got.at[j],
                    send_sem=send1.at[0],
                    recv_sem=recv1.at[j],
                    device_id={"sp": j},
                    device_id_type=MESH,
                ).wait_recv()
            for i in range(per):
                fold[j, i] = jnp.concatenate([state[i], jnp.zeros_like(state[i])], axis=1).astype(BF16)
                both = got[j, i]
                keep, add = both[:, :dim], both[:, dim:].astype(F32)
                sh, sl = halves(state[i])
                state[i] = dot(sh, keep) + dot(sl, keep) + add
        for t in range(count):
            @pl.when(t != me)
            def _(t=t):
                second(t, me).start()
        st_ref[pl.ds(me * per, per)] = fold[me]
        for t in range(count):
            @pl.when(t != me)
            def _(t=t):
                second(t, me).wait_send()

    if workers == count:
        work()
    else:
        pl.when(me < workers)(work)
    for t in range(workers):
        @pl.when(t != me)
        def _(t=t):
            first(t, me).wait_send()
            pltpu.make_async_remote_copy(
                src_ref=fold.at[t],
                dst_ref=st_ref.at[pl.ds(t * per, per)],
                send_sem=send2.at[0],
                recv_sem=recv2.at[t],
                device_id={"sp": t},
                device_id_type=MESH,
            ).wait_recv()


def finish_kernel(head_dim, out_ref, map_ref, st_ref, gain_ref, w_ref, part_ref, mixed):
    @pl.when(pl.program_id(0) == 0)
    def _():
        for h in range(out_ref.shape[1] // head_dim):
            part = slice(h * head_dim, (h + 1) * head_dim)
            states = st_ref[h][:, :head_dim]
            output = out_ref[:, part] + dot(map_ref[:, part], states, (1, 1))
            centered = output - jnp.mean(output, axis=1, keepdims=True)
            spread = jnp.mean(centered * centered, axis=1, keepdims=True)
            mixed[:, part] = (centered * lax.rsqrt(spread + 0.00064) * gain_ref[:, part]).astype(BF16)

    part_ref[...] = dot(mixed[...], w_ref[...]).astype(BF16)


def mixer_branch(query, key, value, step, forget, bias, gain, blender):
    count = lax.axis_size("sp")
    rows, channels = query.shape
    heads = bias.shape[1]
    head_dim = channels // heads
    segment = min(64, rows)
    width = 2 * head_dim
    pairs = heads // 2
    block = pl.BlockSpec((rows, width), lambda p: (0, p))
    out, maps, ka = pl.pallas_call(
        functools.partial(mixer_kernel, head_dim, segment),
        grid=(pairs,),
        in_specs=[block] * 5 + [pl.BlockSpec((rows, heads), lambda p: (0, 0))],
        out_specs=[block, block, pl.BlockSpec((2, head_dim, width), lambda p: (p, 0, 0))],
        out_shape=[
            jax.ShapeDtypeStruct((rows, channels), F32),
            jax.ShapeDtypeStruct((rows, channels), BF16),
            jax.ShapeDtypeStruct((heads, head_dim, width), BF16),
        ],
        compiler_params=pltpu.CompilerParams(vmem_limit_bytes=61 * 1024 * 1024),
    )(query, key, value, step, forget, bias)
    per = max(1, heads // count)
    workers = heads // per
    vmem = pl.BlockSpec(memory_space=pltpu.VMEM)
    states = pl.pallas_call(
        functools.partial(exchange_kernel, count, per, workers),
        out_shape=jax.ShapeDtypeStruct((heads, head_dim, width), BF16),
        in_specs=[vmem],
        out_specs=vmem,
        scratch_shapes=[
            pltpu.VMEM((count, per, head_dim, width), BF16),
            pltpu.VMEM((count, per, head_dim, width), BF16),
            pltpu.SemaphoreType.DMA((count,)),
            pltpu.SemaphoreType.DMA((count,)),
            pltpu.SemaphoreType.DMA((count,)),
            pltpu.SemaphoreType.DMA((count,)),
        ],
        compiler_params=pltpu.CompilerParams(collective_id=1, has_side_effects=True),
    )(ka)
    model_width = blender.shape[1]
    tile = min(512, model_width)
    whole = lambda *shape: pl.BlockSpec(shape, lambda p: (0,) * len(shape))
    return pl.pallas_call(
        functools.partial(finish_kernel, head_dim),
        grid=(model_width // tile,),
        in_specs=[
            whole(rows, channels),
            whole(rows, channels),
            whole(heads, head_dim, width),
            whole(1, channels),
            pl.BlockSpec((channels, tile), lambda p: (0, p)),
        ],
        out_specs=pl.BlockSpec((rows, tile), lambda p: (0, p)),
        out_shape=jax.ShapeDtypeStruct((rows, model_width), BF16),
        scratch_shapes=[pltpu.VMEM((rows, channels), BF16)],
    )(out, maps, states, gain.reshape(1, channels), blender)


def greet(sp_count, tp_count, sp, tp):
    barrier = pltpu.get_barrier_semaphore()
    for d in range(1, sp_count):
        pl.semaphore_signal(
            barrier, inc=1, device_id={"sp": lax.rem(sp + d, sp_count)}, device_id_type=MESH
        )
    for d in range(1, tp_count):
        pl.semaphore_signal(
            barrier, inc=1, device_id={"tp": lax.rem(tp + d, tp_count)}, device_id_type=MESH
        )
    pl.semaphore_wait(barrier, sp_count + tp_count - 2)


def copy_to(src, dst, send, recv, device):
    return pltpu.make_async_remote_copy(
        src_ref=src,
        dst_ref=dst,
        send_sem=send,
        recv_sem=recv,
        device_id=device,
        device_id_type=MESH,
    )


def span(index, size):
    return pl.ds(pl.multiple_of(index * size, size), size)


def row_total(data, terms):
    ones = jnp.ones((8, data.shape[1]), BF16)
    total = None
    for _ in range(terms):
        piece = data.astype(BF16)
        data = data - piece.astype(F32)
        product = dot(ones, piece, (1, 1))
        total = product if total is None else total + product
    return total


def route_kernel(
    sp_count, tp_count, experts, capacity,
    part_ref, skip_ref, gain_ref, ids_ref,
    hidden_ref, slot_ref, rows_ref,
    gathered, squares, outgoing,
    s_part, r_part, s_sq, r_sq, s_out, r_out, s_own, s_fwd, r_col,
):
    sp, tp = lax.axis_index("sp"), lax.axis_index("tp")
    rows, model = part_ref.shape
    cols = model // tp_count
    mine = span(tp, cols)
    groups = tp_count // 2
    core, group = lax.rem(tp, 2), tp // 2
    sibling = group * 2 + 1 - core
    greet(sp_count, tp_count, sp, tp)

    def part_copy(p):
        return copy_to(
            part_ref.at[:, span(p, cols)], gathered.at[tp], s_part.at[p], r_part.at[tp], {"tp": p}
        )

    for d in range(1, tp_count):
        part_copy(lax.rem(tp + d, tp_count)).start()

    ids = ids_ref[...]
    top = ids.shape[1]
    lanes = lax.broadcasted_iota(jnp.int32, (rows, experts), 1)
    named = [ids[:, k : k + 1] == lanes for k in range(top)]
    anyone = sum(jnp.where(n, 1.0, 0.0) for n in named).astype(BF16)
    r0 = lax.broadcasted_iota(jnp.int32, (rows, rows), 0)
    r1 = lax.broadcasted_iota(jnp.int32, (rows, rows), 1)
    before = dot(jnp.where(r0 > r1, 1.0, 0.0).astype(BF16), anyone)
    slots = [
        jnp.sum(
            jnp.where(n, before + lanes.astype(F32) * capacity, 0.0), axis=1, keepdims=True
        ).astype(jnp.int32)
        for n in named
    ]
    slot_ref[...] = jnp.concatenate(slots, axis=1)

    branch = part_ref[:, mine].astype(F32)
    for d in range(1, tp_count):
        p = lax.rem(tp + d, tp_count)
        copy_to(gathered.at[p], gathered.at[p], s_part.at[p], r_part.at[p], {"tp": p}).wait_recv()
        branch = branch + gathered[p].astype(F32)
    hidden = skip_ref[:, mine].astype(F32) + branch
    hidden_ref[...] = hidden
    squares[tp] = row_total(hidden * hidden, 3)

    def square_copy(p):
        return copy_to(squares.at[tp], squares.at[tp], s_sq.at[p], r_sq.at[tp], {"tp": p})

    for d in range(1, tp_count):
        square_copy(lax.rem(tp + d, tp_count)).start()
    total = squares[tp]
    for d in range(1, tp_count):
        p = lax.rem(tp + d, tp_count)
        copy_to(squares.at[p], squares.at[p], s_sq.at[p], r_sq.at[p], {"tp": p}).wait_recv()
        total = total + squares[p]
    inverse = lax.rsqrt(total / model + 1e-06)
    first = jnp.where(lax.broadcasted_iota(jnp.int32, (8, 128), 0) == 0, 1.0, 0.0).astype(BF16)
    column = None
    for _ in range(3):
        piece = inverse.astype(BF16)
        inverse = inverse - piece.astype(F32)
        product = dot(piece, first, (0, 0))
        column = product if column is None else column + product
    normed = (hidden * column[:, :1] * gain_ref[:, mine]).astype(BF16)

    per = experts // sp_count * capacity
    places = lax.broadcasted_iota(jnp.int32, (rows, per), 1)

    def block_for(t):
        at = places + t * per
        chosen = (slots[0] == at)
        for s in slots[1:]:
            chosen = chosen | (s == at)
        return dot(jnp.where(chosen, 1.0, 0.0).astype(BF16), normed, (0, 0)).astype(BF16)

    def out_copy(t):
        return copy_to(
            outgoing.at[t], rows_ref.at[sp, :, mine], s_out.at[t], r_out.at[sp], {"sp": t}
        )

    def give(d, carry):
        t = lax.rem(sp + d, sp_count)
        outgoing[t] = block_for(t)
        out_copy(t).start()
        return carry

    lax.fori_loop(1, sp_count, give, 0)
    rows_ref[sp, :, mine] = block_for(sp)

    def own_copy(p, s):
        here = rows_ref.at[s, :, mine]
        return copy_to(here, here, s_own.at[p, s], r_col.at[tp, s], {"tp": p})

    def forward(o, s):
        here = rows_ref.at[s, :, span(o, cols)]
        return copy_to(here, here, s_fwd.at[o, s], r_col.at[o, s], {"tp": sibling})

    def arrived(o, s):
        here = rows_ref.at[s, :, span(o, cols)]
        copy_to(here, here, s_fwd.at[o, s], r_col.at[o, s], {"tp": sibling}).wait_recv()

    def peers():
        return [lax.rem(group + g, groups) * 2 + core for g in range(1, groups)]

    lag = 2

    def relay(d, carry):
        @pl.when(d < sp_count)
        def _():
            s = lax.rem(sp - d + sp_count, sp_count)

            @pl.when(d > 0)
            def _():
                here = rows_ref.at[s, :, mine]
                copy_to(here, here, s_out.at[s], r_out.at[s], {"sp": s}).wait_recv()

            for p in peers():
                own_copy(p, s).start()
            own_copy(sibling, s).start()

        @pl.when(d >= lag)
        def _():
            s = lax.rem(sp - (d - lag) + sp_count, sp_count)
            for o in peers():
                arrived(o, s)
                forward(o, s).start()

        return carry

    lax.fori_loop(0, sp_count + lag, relay, 0)

    def settle(s, carry):
        arrived(sibling, s)
        for g in range(1, groups):
            arrived(lax.rem(group + g, groups) * 2 + 1 - core, s)
        own_copy(sibling, s).wait_send()
        for p in peers():
            own_copy(p, s).wait_send()
            forward(p, s).wait_send()
        return carry

    lax.fori_loop(0, sp_count, settle, 0)

    def sent(d, carry):
        out_copy(lax.rem(sp + d, sp_count)).wait_send()
        return carry

    lax.fori_loop(1, sp_count, sent, 0)
    for d in range(1, tp_count):
        p = lax.rem(tp + d, tp_count)
        part_copy(p).wait_send()
        square_copy(p).wait_send()


def return_kernel(
    sp_count, tp_count,
    rows_ref, switch_ref, expand_ref, contract_ref, hidden_ref, slot_ref, weight_ref,
    out_ref,
    y_ref, from_sib, pair, from_peer, summed, back,
    s_sib, r_sib, s_peer, r_peer, s_back, r_back, s_own, s_fwd, r_col,
):
    sp, tp = lax.axis_index("sp"), lax.axis_index("tp")
    per, model = y_ref.shape[1:]
    rows = hidden_ref.shape[0]
    cols = model // tp_count
    mine = span(tp, cols)
    groups = tp_count // 2
    core, group = lax.rem(tp, 2), tp // 2
    sibling = group * 2 + 1 - core
    greet(sp_count, tp_count, sp, tp)

    def sib_copy(s, g):
        return copy_to(
            y_ref.at[s, :, span(g * 2 + 1 - core, cols)],
            from_sib.at[s, g],
            s_sib.at[s, g],
            r_sib.at[s, g],
            {"tp": sibling},
        )

    def peer_copy(s, g):
        return copy_to(
            pair.at[s, g],
            from_peer.at[s, group],
            s_peer.at[s, g],
            r_peer.at[s, group],
            {"tp": g * 2 + core},
        )

    def back_copy(t):
        return copy_to(summed.at[t], back.at[sp], s_back.at[t], r_back.at[sp], {"sp": t})

    def others():
        return [lax.rem(group + d, groups) for d in range(1, groups)]

    def order(d):
        return lax.rem(sp + 1 + d, sp_count)

    local = switch_ref.shape[0]
    capacity = per // local
    chunk = math.gcd(sp_count, max(1, 256 // capacity))
    chunks = sp_count // chunk

    def expert(i):
        at = [order(i * chunk + c) for c in range(chunk)]
        for e in range(local):
            inside = slice(e * capacity, (e + 1) * capacity)
            data = jnp.concatenate([rows_ref[s, inside, :] for s in at], axis=0)
            gate = dot(data, switch_ref[e])
            units = (gate / (1.0 + jnp.exp(-gate)) * dot(data, expand_ref[e])).astype(BF16)
            value = dot(units, contract_ref[e]).astype(BF16)
            for c in range(chunk):
                y_ref[at[c], inside, :] = value[c * capacity : (c + 1) * capacity]
        for s in at:
            for g in others():
                sib_copy(s, g).start()
            sib_copy(s, group).start()

    def meet(s):
        for g in others():
            sib_copy(s, g).wait_recv()
            pair[s, g] = (
                y_ref[s, :, span(g * 2 + core, cols)].astype(F32) + from_sib[s, g].astype(F32)
            ).astype(BF16)
            peer_copy(s, g).start()
        sib_copy(s, group).wait_recv()

    def total_up(s):
        total = y_ref[s, :, mine].astype(F32) + from_sib[s, group].astype(F32)
        for g in others():
            copy_to(
                from_peer.at[s, g],
                from_peer.at[s, g],
                s_peer.at[s, g],
                r_peer.at[s, g],
                {"tp": g * 2 + core},
            ).wait_recv()
            total = total + from_peer[s, g].astype(F32)

        @pl.when(s != sp)
        def _():
            summed[s] = total.astype(BF16)
            back_copy(s).start()

        @pl.when(s == sp)
        def _():
            back[s] = total.astype(BF16)

    def step(i, carry):
        @pl.when(i < chunks)
        def _():
            expert(i)

        @pl.when((i >= 1) & (i <= chunks))
        def _():
            for c in range(chunk):
                meet(order((i - 1) * chunk + c))

        @pl.when(i >= 2)
        def _():
            for c in range(chunk):
                total_up(order((i - 2) * chunk + c))

        return carry

    lax.fori_loop(0, chunks + 2, step, 0)
    slots = slot_ref[...]
    weights = weight_ref[...]
    places = lax.broadcasted_iota(jnp.int32, (rows, sp_count * per), 1)
    top = slots.shape[1]
    chosen = [jnp.where(slots[:, k : k + 1] == places, 1.0, 0.0).astype(BF16) for k in range(top)]

    def landed(d, carry):
        s = lax.rem(sp + d, sp_count)
        copy_to(back.at[s], back.at[s], s_back.at[s], r_back.at[s], {"sp": s}).wait_recv()
        return carry

    lax.fori_loop(1, sp_count, landed, 0)
    returned = back[...].reshape(sp_count * per, cols)
    result = hidden_ref[...] + sum(
        weights[:, k : k + 1] * dot(chosen[k], returned) for k in range(top)
    )
    out_ref[:, mine] = result.astype(BF16)

    def own_copy(p):
        here = out_ref.at[:, mine]
        return copy_to(here, here, s_own.at[p], r_col.at[tp], {"tp": p})

    def forward(o):
        here = out_ref.at[:, span(o, cols)]
        return copy_to(here, here, s_fwd.at[o], r_col.at[o], {"tp": sibling})

    peers = [g * 2 + core for g in others()]
    for p in peers:
        own_copy(p).start()
    own_copy(sibling).start()
    for p in peers:
        forward(p).wait_recv()
        forward(p).start()
    forward(sibling).wait_recv()
    for g in others():
        forward(g * 2 + 1 - core).wait_recv()
    own_copy(sibling).wait_send()
    for p in peers:
        own_copy(p).wait_send()
        forward(p).wait_send()

    def close(s, carry):
        sib_copy(s, group).wait_send()
        for g in others():
            sib_copy(s, g).wait_send()
            peer_copy(s, g).wait_send()
        return carry

    lax.fori_loop(0, sp_count, close, 0)

    def sent(d, carry):
        back_copy(lax.rem(sp + d, sp_count)).wait_send()
        return carry

    lax.fori_loop(1, sp_count, sent, 0)


def body(
    readout_query_vectors,
    attention_key_vectors,
    attention_content_vectors,
    step_size_preactivation,
    forgetting_preactivation,
    extra_forgetting_bias,
    subspace_normalizer_gain,
    skip_connection_stream,
    blender_projection_matrix,
    specialist_prenormal_gain,
    cluster_router_chance,
    specialist_chance_within_cluster,
    chosen_specialist_ids,
    specialist_switch_matrix,
    specialist_expansion_matrix,
    specialist_contraction_matrix,
):
    partial_branch = mixer_branch(
        readout_query_vectors,
        attention_key_vectors,
        attention_content_vectors,
        step_size_preactivation,
        forgetting_preactivation,
        extra_forgetting_bias,
        subspace_normalizer_gain,
        blender_projection_matrix,
    )
    tok_rows, model_width = skip_connection_stream.shape
    sp_count, tp_count = lax.axis_size("sp"), lax.axis_size("tp")
    local_experts = specialist_switch_matrix.shape[0]
    experts = local_experts * sp_count
    top_count = chosen_specialist_ids.shape[1]
    capacity = 2 * tok_rows * top_count // experts
    cols = model_width // tp_count
    per = local_experts * capacity
    groups = tp_count // 2
    vmem = pl.BlockSpec(memory_space=pltpu.VMEM)
    sems = pltpu.SemaphoreType.DMA
    hidden_cols, slots, rows_in = pl.pallas_call(
        functools.partial(route_kernel, sp_count, tp_count, experts, capacity),
        out_shape=[
            jax.ShapeDtypeStruct((tok_rows, cols), F32),
            jax.ShapeDtypeStruct((tok_rows, top_count), jnp.int32),
            jax.ShapeDtypeStruct((sp_count, per, model_width), BF16),
        ],
        in_specs=[vmem] * 4,
        out_specs=[vmem] * 3,
        scratch_shapes=[
            pltpu.VMEM((tp_count, tok_rows, cols), BF16),
            pltpu.VMEM((tp_count, 8, tok_rows), F32),
            pltpu.VMEM((sp_count, per, cols), BF16),
            sems((tp_count,)),
            sems((tp_count,)),
            sems((tp_count,)),
            sems((tp_count,)),
            sems((sp_count,)),
            sems((sp_count,)),
            sems((tp_count, sp_count)),
            sems((tp_count, sp_count)),
            sems((tp_count, sp_count)),
        ],
        compiler_params=pltpu.CompilerParams(
            collective_id=2, has_side_effects=True, vmem_limit_bytes=40 * 1024 * 1024
        ),
    )(
        partial_branch,
        skip_connection_stream,
        specialist_prenormal_gain.reshape(1, model_width),
        chosen_specialist_ids,
    )
    route_weight = (
        cluster_router_chance[:, None]
        * specialist_chance_within_cluster
        / jnp.sum(specialist_chance_within_cluster, axis=1, keepdims=True)
    )
    return pl.pallas_call(
        functools.partial(return_kernel, sp_count, tp_count),
        out_shape=jax.ShapeDtypeStruct((tok_rows, model_width), BF16),
        in_specs=[vmem] * 7,
        out_specs=vmem,
        scratch_shapes=[
            pltpu.VMEM((sp_count, per, model_width), BF16),
            pltpu.VMEM((sp_count, groups, per, cols), BF16),
            pltpu.VMEM((sp_count, groups, per, cols), BF16),
            pltpu.VMEM((sp_count, groups, per, cols), BF16),
            pltpu.VMEM((sp_count, per, cols), BF16),
            pltpu.VMEM((sp_count, per, cols), BF16),
            sems((sp_count, groups)),
            sems((sp_count, groups)),
            sems((sp_count, groups)),
            sems((sp_count, groups)),
            sems((sp_count,)),
            sems((sp_count,)),
            sems((tp_count,)),
            sems((tp_count,)),
            sems((tp_count,)),
        ],
        compiler_params=pltpu.CompilerParams(
            collective_id=3, has_side_effects=True, vmem_limit_bytes=50 * 1024 * 1024
        ),
    )(
        rows_in,
        specialist_switch_matrix,
        specialist_expansion_matrix,
        specialist_contraction_matrix,
        hidden_cols,
        slots,
        route_weight,
    )


def solution(mesh):
    in_specs = (
        P("sp", "tp"),
        P("sp", "tp"),
        P("sp", "tp"),
        P("sp", "tp"),
        P("sp", "tp"),
        P("sp", "tp"),
        P("tp"),
        P("sp", None),
        P("tp", None),
        P(),
        P("sp"),
        P("sp", None),
        P("sp", None),
        P("sp", None, "tp"),
        P("sp", None, "tp"),
        P("sp", "tp", None),
    )
    out_specs = P("sp", None)
    return jax.shard_map(body, mesh=mesh, in_specs=in_specs, out_specs=out_specs, check_vma=False)
```
